32 devices in a mesh: grp: 2 (over y), sp: 4 (over z), tp: 4 (over x, core).
Axes of the slice: x: 2, y: 2, z: 4, core: 2. Of those that a mesh axis runs over, the one named last changes fastest.
Arguments:
- residual: bfloat16 [2048, 2048], P(('grp', 'sp', 'tp')), parts along dimension 0, may hold values from -6 to 6
- queries_wide: bfloat16 [2048, 1024], P(('grp', 'sp'), 'tp'), parts along dimension 0, may hold values from -6 to 6
- keys_wide: bfloat16 [2048, 512], P(('grp', 'sp'), 'tp'), parts along dimension 0, may hold values from -6 to 6
- values_wide: bfloat16 [2048, 512], P(('grp', 'sp'), 'tp'), parts along dimension 0, may hold values from -6 to 6
- queries_narrow: bfloat16 [2048, 512], P(('grp', 'sp'), 'tp'), parts along dimension 0, may hold values from -6 to 6
- keys_narrow: bfloat16 [2048, 256], P(('grp', 'sp'), 'tp'), parts along dimension 0, may hold values from -6 to 6
- values_narrow: bfloat16 [2048, 256], P(('grp', 'sp'), 'tp'), parts along dimension 0, may hold values from -6 to 6
- query_gain_wide: float32 [128], replicated, may hold values from 1 to 6
- key_gain_wide: float32 [128], replicated, may hold values from 1 to 6
- query_gain_narrow: float32 [64], replicated, may hold values from 1 to 6
- key_gain_narrow: float32 [64], replicated, may hold values from 1 to 6
- output_wide: bfloat16 [1024, 2048], P('tp'), may hold values from -0.3125 to 0.3125
- output_narrow: bfloat16 [512, 2048], P('tp'), may hold values from -0.3125 to 0.3125
- norm_gain: float32 [2048], replicated, may hold values from 0.1 to 1.9
- gate_weight: bfloat16 [4, 2048, 3584], P('sp', None, 'tp'), may hold values from -0.125 to 0.125
- up_weight: bfloat16 [4, 2048, 3584], P('sp', None, 'tp'), may hold values from -0.125 to 0.125
- down_weight: bfloat16 [4, 3584, 2048], P('sp', 'tp'), may hold values from -0.09375 to 0.09375
- route_ids: int32 [2048, 2], P(('grp', 'sp', 'tp')), parts along dimension 0, may hold values from 0 to 3, all different within a row; in each aligned block of 64 rows (0 to 63, 64 to 127, ...) at most 64 rows name the same one
- route_weights: float32 [2048, 2], P(('grp', 'sp', 'tp')), parts along dimension 0, may hold values from 0.1 to 0.9
Outputs:
- result: bfloat16 [2048, 2048], P(('grp', 'sp', 'tp')), parts along dimension 0
The draws below stay inside these ranges and needn't reach their ends.
There are 2 independent parts, one for each index of `grp`. The reference program is written for one: setup_inputs(seed, part) draws one part's arguments, and reference() takes and returns one part's arrays. A program takes and returns all parts, laid end to end along the dimension named above; an argument that names none is the same for every part. Nothing has to cross between parts.
Inputs may be any that keep to these rules, and one draw needn't show every extreme that they name: `route_ids`: in each aligned block of 64 rows (the rows of one device) no expert is named by more than 64 rows, a bound that some block reaches; a row names 2 different experts.
All inputs are finite; a program needn't handle non-finite values.
Results may differ from the reference program's by a relative error of at most 0.013.
The reference program's roundings to bfloat16 on the way count: a program that leaves them out, or rounds other values in their place, can miss the bound.
Values may be sent and summed in bfloat16 or wider, within the bound.
No kernel may reach another device: no remote copies, remote signals or barrier semaphores. Data moves between devices by JAX's collectives and lax.ppermute only.
A program may use at most 128 MiB of HBM per device.

```python
import math
import jax
import jax.numpy as jnp
import numpy as np
from jax import lax

D = 2048
HW = 8
KW = 4
DW = 128
HN = 8
KN = 4
DN = 64
FF = 3584
TOPK = 2
GRID = 64
TOKENS = 1024
ROWS = 64
EXPERTS = 4
CAP = 64
N_SP = 4
N_TP = 4


def draw_field(key, tag, head_count, head_width):
    noise_key = jax.random.fold_in(key, tag)
    field = jax.random.normal(noise_key, (TOKENS, head_count, head_width), jnp.float32)
    field = jnp.clip(field, -6.0, 6.0)
    return field.reshape(TOKENS, head_count * head_width).astype(jnp.bfloat16)


def draw_gain(key, tag, head_width):
    base_key = jax.random.fold_in(key, tag)
    return jax.random.uniform(base_key, (head_width,), jnp.float32, 1.0, 2.2)


def draw_queries_wide(key, part):
    return draw_field(key, 101, HW, DW)


def draw_keys_wide(key, part):
    return draw_field(key, 102, KW, DW)


def draw_queries_narrow(key, part):
    return draw_field(key, 103, HN, DN)


def draw_keys_narrow(key, part):
    return draw_field(key, 104, KN, DN)


def draw_query_gain_wide(key, part):
    return draw_gain(key, 201, DW)


def draw_key_gain_wide(key, part):
    return draw_gain(key, 202, DW)


def draw_query_gain_narrow(key, part):
    return draw_gain(key, 203, DN)


def draw_key_gain_narrow(key, part):
    return draw_gain(key, 204, DN)


def block_scale(key, dims, split, smallest, largest):
    gain = 1.0
    for dim, shards_of in split:
        heights = jax.random.uniform(jax.random.fold_in(jax.random.fold_in(key, 6), dim), (shards_of,), jnp.float32, smallest / len(split), largest / len(split))
        gain = gain * jnp.repeat(jnp.exp(heights), dims[dim] // shards_of).reshape((-1,) + (1,) * (len(dims) - 1 - dim))
    return gain


def shared_out(stream_key, own, number, rows, count, top, limit, skew):
    sequence = jax.random.permutation(stream_key, count)
    packed, usual = shares(count, rows * top, limit, skew, True), shares(count, rows * top, limit, skew, False)
    places = jnp.arange(count)

    def named(sizes, rotation):
        used = int((sizes > 0).sum())
        fixed = max(1, used // 4)
        moved = fixed + (places - fixed + rotation * (used - fixed)) % max(1, count - fixed)
        return jnp.zeros((count,), jnp.int32).at[sequence[jnp.where(places < fixed, places, moved)]].set(jnp.asarray(sizes, jnp.int32))

    sizes = jnp.where(number % 4 == 0, named(packed, number // 4), named(usual, number - number // 4 - 1))
    mixed = jax.random.permutation(jax.random.fold_in(own, 3), count)
    source_of, receiver = mixed[0:count // 2 * 2:2], mixed[1:count // 2 * 2:2]
    margin = jnp.minimum(sizes[source_of] - 1, limit - sizes[receiver]) // 2
    margin = jnp.where((source_of == sequence[0]) | (receiver == sequence[0]) | (sizes[receiver] == 0), 0, jnp.maximum(margin, 0))
    moved = jax.random.randint(jax.random.fold_in(own, 4), (count // 2,), 0, 1 << 20) % (margin + 1)
    sizes = sizes.at[source_of].add(-moved).at[receiver].add(moved)
    items = jnp.searchsorted(jnp.cumsum(sizes), jnp.arange(rows * top), side="right").astype(jnp.int32)
    grid = items.reshape(top, rows).T
    grid = grid[jax.random.permutation(jax.random.fold_in(own, 1), rows)]
    rotation = jax.random.randint(jax.random.fold_in(own, 2), (rows, 1), 0, top)
    return jnp.take_along_axis(grid, (jnp.arange(top)[None, :] + rotation) % top, axis=1)


def shares(amount, total, bound, slope, full):
    portions = [(1 << 20) // math.isqrt(grade ** slope) + 1 for grade in range(1, amount + 1)]
    largest = bound if full else min(bound, max(-(-total // amount), total * portions[0] // sum(portions)))
    least = 1 if total - largest >= amount - 1 else 0
    counts, spare = [largest] + [least] * (amount - 1), total - largest - least * (amount - 1)
    while spare > 0:
        candidates = [i for i in range(1, amount) if counts[i] < largest] or [i for i in range(1, amount) if counts[i] < bound]
        mass, left = sum([portions[i] for i in candidates]), spare
        for i in candidates:
            more = min(bound - counts[i], max(1, left * portions[i] // mass), spare)
            counts[i] = counts[i] + more
            spare = spare - more
    return np.array(counts)


def noise(rng, shape, width, reach, split=(), kind=jnp.bfloat16):
    level = block_scale(rng, shape, split, -0.22, 0.18) if split else 1.0
    result = jax.random.normal(rng, shape, jnp.float32) * width * level
    return jnp.minimum(jnp.maximum(result, -reach), reach).astype(kind)


def setup_inputs(seed: int = 0, part: int = 0) -> dict:
    splits = jax.random.split(jax.random.key(seed), 20)
    part_splits = jax.random.split(jax.random.fold_in(splits[19], part), 20)
    residual = noise(part_splits[0], (TOKENS, D), 1.0, 6.0, ((0, 16),))
    queries_wide = draw_queries_wide(jax.random.fold_in(jax.random.fold_in(splits[19], part), 71), part)
    keys_wide = draw_keys_wide(jax.random.fold_in(jax.random.fold_in(splits[19], part), 71), part)
    values_wide = noise(part_splits[3], (TOKENS, KW * DW), 1.0, 6.0, ((0, 4), (1, 4)))
    queries_narrow = draw_queries_narrow(jax.random.fold_in(jax.random.fold_in(splits[19], part), 71), part)
    keys_narrow = draw_keys_narrow(jax.random.fold_in(jax.random.fold_in(splits[19], part), 71), part)
    values_narrow = noise(part_splits[6], (TOKENS, KN * DN), 1.0, 6.0, ((0, 4), (1, 4)))
    query_gain_wide = draw_query_gain_wide(jax.random.fold_in(splits[19], 71), part)
    key_gain_wide = draw_key_gain_wide(jax.random.fold_in(splits[19], 71), part)
    query_gain_narrow = draw_query_gain_narrow(jax.random.fold_in(splits[19], 71), part)
    key_gain_narrow = draw_key_gain_narrow(jax.random.fold_in(splits[19], 71), part)
    output_wide = noise(splits[11], (HW * DW, D), ((HW * DW + HN * DN) // 4) ** -0.5, 0.3125, ((0, 4),))
    output_narrow = noise(splits[12], (HN * DN, D), ((HW * DW + HN * DN) // 4) ** -0.5, 0.3125, ((0, 4),))
    norm_gain = jnp.clip(1.0 + 0.18 * jax.random.normal(splits[13], (D,), jnp.float32), 0.1, 1.9)
    gate_weight = noise(splits[14], (EXPERTS, D, FF), D ** -0.5, 0.125, ((0, 4), (2, 4)))
    up_weight = noise(splits[15], (EXPERTS, D, FF), D ** -0.5, 0.125, ((0, 4), (2, 4)))
    down_weight = noise(splits[16], (EXPERTS, FF, D), FF ** -0.5, 0.09375, ((0, 4), (1, 4)))
    route_ids_keys = jax.random.split(jax.random.fold_in(part_splits[17], 1), TOKENS // ROWS)
    route_ids_turns = jax.random.permutation(jax.random.fold_in(part_splits[17], 3), TOKENS // ROWS)
    route_ids = jax.vmap(lambda own, number: shared_out(jax.random.fold_in(part_splits[17], 2), own, number, ROWS, EXPERTS, TOPK, CAP, 2))(route_ids_keys, route_ids_turns).reshape((TOKENS, TOPK))
    route_weights = jnp.clip(0.1 + 0.79999997 * jax.random.uniform(part_splits[18], (TOKENS, TOPK), jnp.float32) ** block_scale(part_splits[18], (TOKENS, TOPK), ((0, 16),), -0.2, 0.2), 0.1, 0.9)
    return {"residual": residual, "queries_wide": queries_wide, "keys_wide": keys_wide, "values_wide": values_wide, "queries_narrow": queries_narrow, "keys_narrow": keys_narrow, "values_narrow": values_narrow, "query_gain_wide": query_gain_wide, "key_gain_wide": key_gain_wide, "query_gain_narrow": query_gain_narrow, "key_gain_narrow": key_gain_narrow, "output_wide": output_wide, "output_narrow": output_narrow, "norm_gain": norm_gain, "gate_weight": gate_weight, "up_weight": up_weight, "down_weight": down_weight, "route_ids": route_ids, "route_weights": route_weights}


THETA = 10000.0
EPS = 1e-06

def rotary_tables(places, head_width):
    quarter = head_width // 4
    inv_freq = THETA ** (-jnp.arange(quarter, dtype=jnp.float32) / quarter)
    grid_rows = (places // GRID).astype(jnp.float32)
    grid_cols = (places % GRID).astype(jnp.float32)
    row_angle = grid_rows[:, None] * inv_freq[None, :]
    col_angle = grid_cols[:, None] * inv_freq[None, :]
    angles = jnp.concatenate([row_angle, row_angle, col_angle, col_angle], axis=-1)
    return (jnp.cos(angles), jnp.sin(angles))

def head_norm_rotate(values, gain_vec, cos_table, sin_table):
    as_float = values.astype(jnp.float32)
    scaled = as_float * lax.rsqrt(lax.optimization_barrier(jnp.mean(as_float * as_float, axis=-1, keepdims=True)) + EPS)
    scaled = scaled * gain_vec.astype(jnp.float32)
    full_shape = scaled.shape
    quarter = full_shape[-1] // 4
    halves = scaled.reshape(full_shape[:-1] + (2, 2, quarter))
    turned = jnp.stack([-halves[..., 1, :], halves[..., 0, :]], axis=-2).reshape(full_shape)
    return (scaled * cos_table[:, None, :] + turned * sin_table[:, None, :]).astype(jnp.bfloat16)

def rounded(values):
    return lax.optimization_barrier(values.astype(jnp.bfloat16)).astype(jnp.float32)

def attend(queries, keys, values, key_heads):
    token_count = queries.shape[0]
    head_width = queries.shape[2]
    group_size = queries.shape[1] // key_heads
    block_len = math.gcd(token_count, 512)
    grouped = queries.reshape(token_count // block_len, block_len, key_heads, group_size, head_width)
    keys_float = keys.reshape(token_count, key_heads, head_width).astype(jnp.float32)
    values_float = values.reshape(token_count, key_heads, head_width).astype(jnp.float32)
    score_scale = head_width ** (-0.5)

    def one_block(query_block):
        scores = jnp.einsum('qhgd,khd->hgqk', query_block.astype(jnp.float32), keys_float) * score_scale
        row_max = lax.optimization_barrier(jnp.max(scores, axis=-1, keepdims=True))
        weights = jnp.exp(scores - row_max)
        weight_sum = lax.optimization_barrier(jnp.sum(weights, axis=-1))
        mixed_values = jnp.einsum('hgqk,khd->qhgd', rounded(weights), values_float)
        return (mixed_values / jnp.transpose(weight_sum, (2, 0, 1))[..., None]).astype(jnp.bfloat16)
    heads_out = lax.map(one_block, grouped)
    return heads_out.reshape(token_count, key_heads * group_size * head_width)

def reference(residual, queries_wide, keys_wide, values_wide, queries_narrow, keys_narrow, values_narrow, query_gain_wide, key_gain_wide, query_gain_narrow, key_gain_narrow, output_wide, output_narrow, norm_gain, gate_weight, up_weight, down_weight, route_ids, route_weights):
    places = jnp.arange(TOKENS, dtype=jnp.int32)
    cos_wide, sin_wide = rotary_tables(places, DW)
    cos_narrow, sin_narrow = rotary_tables(places, DN)
    q_wide = head_norm_rotate(queries_wide.reshape(TOKENS, HW, DW), query_gain_wide, cos_wide, sin_wide)
    k_wide = head_norm_rotate(keys_wide.reshape(TOKENS, KW, DW), key_gain_wide, cos_wide, sin_wide)
    q_narrow = head_norm_rotate(queries_narrow.reshape(TOKENS, HN, DN), query_gain_narrow, cos_narrow, sin_narrow)
    k_narrow = head_norm_rotate(keys_narrow.reshape(TOKENS, KN, DN), key_gain_narrow, cos_narrow, sin_narrow)
    heads_wide = attend(q_wide, k_wide, values_wide, KW)
    heads_narrow = attend(q_narrow, k_narrow, values_narrow, KN)
    wide_cols = HW * DW // N_TP
    narrow_cols = HN * DN // N_TP
    summed = jnp.zeros((TOKENS, D), jnp.float32)
    for shard_index in range(N_TP):
        wide_lo = shard_index * wide_cols
        narrow_lo = shard_index * narrow_cols
        shard_term = jnp.dot(heads_wide[:, wide_lo:wide_lo + wide_cols], output_wide[wide_lo:wide_lo + wide_cols], preferred_element_type=jnp.float32)
        shard_term = shard_term + jnp.dot(heads_narrow[:, narrow_lo:narrow_lo + narrow_cols], output_narrow[narrow_lo:narrow_lo + narrow_cols], preferred_element_type=jnp.float32)
        summed = summed + rounded(shard_term)
    state_float = rounded(residual.astype(jnp.float32) + summed)
    normed = (state_float * lax.rsqrt(lax.optimization_barrier(jnp.mean(state_float * state_float, axis=-1, keepdims=True)) + EPS) * norm_gain.astype(jnp.float32)).astype(jnp.bfloat16)
    flat_ids = route_ids.reshape(-1)
    flat_weights = route_weights.reshape(-1)
    room = N_SP * N_TP * CAP
    shard_cols = FF // N_TP

    def expert_step(carried, expert):
        gate_one, up_one, down_one, number = expert
        ordering = jnp.argsort((flat_ids != number).astype(jnp.int32), stable=True)[:room].astype(jnp.int32)
        live_slot = flat_ids[ordering] == number
        owner_row = ordering // TOPK
        picked = normed[owner_row]
        gate_act = jnp.dot(picked, gate_one, preferred_element_type=jnp.float32)
        up_act = jnp.dot(picked, up_one, preferred_element_type=jnp.float32)
        hidden = (jax.nn.silu(gate_act) * up_act).astype(jnp.bfloat16)
        summed_out = jnp.zeros((room, D), jnp.float32)
        for shard_index in range(N_TP):
            low = shard_index * shard_cols
            partial_value = jnp.dot(hidden[:, low:low + shard_cols], down_one[low:low + shard_cols], preferred_element_type=jnp.float32)
            summed_out = summed_out + rounded(partial_value)
        expert_out = rounded(summed_out)
        weight = jnp.where(live_slot, flat_weights[ordering], 0.0)
        return (carried.at[owner_row].add(weight[:, None] * expert_out), None)
    mixture, _ = lax.scan(expert_step, jnp.zeros((TOKENS, D), jnp.float32), (gate_weight, up_weight, down_weight, jnp.arange(EXPERTS, dtype=jnp.int32)))
    return (state_float + mixture).astype(jnp.bfloat16)
```

```python
import functools

import jax
import jax.numpy as jnp
import numpy as np
from jax import lax
from jax.experimental import pallas as pl
from jax.experimental.pallas import tpu as pltpu
from jax.sharding import PartitionSpec as P

GRID = 64


THETA = 10000.0
EPS = 1e-06
NEG_BIG = -1e30


def rotary_tables(places, head_width):
    quarter = head_width // 4
    inv_freq = THETA ** (-jnp.arange(quarter, dtype=jnp.float32) / quarter)
    grid_rows = (places // GRID).astype(jnp.float32)
    grid_cols = (places % GRID).astype(jnp.float32)
    row_angle = grid_rows[:, None] * inv_freq[None, :]
    col_angle = grid_cols[:, None] * inv_freq[None, :]
    angles = jnp.concatenate([row_angle, row_angle, col_angle, col_angle], axis=-1)
    return (jnp.cos(angles), jnp.sin(angles))


def head_norm_rotate(values, gain_vec, cos_table, sin_table):
    as_float = values.astype(jnp.float32)
    scaled = as_float * lax.rsqrt(jnp.mean(as_float * as_float, axis=-1, keepdims=True) + EPS)
    scaled = scaled * gain_vec
    full_shape = scaled.shape
    quarter = full_shape[-1] // 4
    halves = scaled.reshape(full_shape[:-1] + (2, 2, quarter))
    turned = jnp.stack([-halves[..., 1, :], halves[..., 0, :]], axis=-2).reshape(full_shape)
    return (scaled * cos_table[:, None, :] + turned * sin_table[:, None, :]).astype(jnp.bfloat16)


def fresh_state(queries):
    key_heads, group_size, tok_count = (queries.shape[1], queries.shape[2], queries.shape[0])
    return (
        jnp.full((key_heads, group_size, tok_count), NEG_BIG, jnp.float32),
        jnp.zeros((key_heads, group_size, tok_count), jnp.float32),
        jnp.zeros(queries.shape, jnp.float32),
    )


def key_sweep(carried, queries, keys, values):
    key_count = keys.shape[0]
    key_heads = queries.shape[1]
    head_width = queries.shape[3]
    block_len = 2048 if key_count % 2048 == 0 else key_count
    key_blocks = keys.reshape(key_count // block_len, block_len, key_heads, head_width)
    value_blocks = values.reshape(key_count // block_len, block_len, key_heads, head_width)
    score_scale = head_width ** (-0.5)

    def step(carried_state, blocks_in):
        key_block, value_block = blocks_in
        running_max, weight_sum, weighted = carried_state
        scores = (
            jnp.einsum("qhgd,khd->hgqk", queries, key_block, preferred_element_type=jnp.float32)
            * score_scale
        )
        new_max = jnp.maximum(running_max, jnp.max(scores, axis=-1))
        weights = jnp.exp(scores - new_max[..., None])
        rescale = jnp.exp(running_max - new_max)
        weight_sum = weight_sum * rescale + jnp.sum(weights, axis=-1)
        mixed_values = jnp.einsum(
            "hgqk,khd->qhgd",
            weights.astype(jnp.bfloat16),
            value_block,
            preferred_element_type=jnp.float32,
        )
        weighted = weighted * jnp.transpose(rescale, (2, 0, 1))[..., None] + mixed_values
        return ((new_max, weight_sum, weighted), None)

    carried, _ = lax.scan(step, carried, (key_blocks, value_blocks))
    return carried


def finish_heads(carried):
    weighted = carried[2]
    outcome = weighted / jnp.transpose(carried[1], (2, 0, 1))[..., None]
    return outcome.astype(jnp.bfloat16).reshape(weighted.shape[0], -1)


def slot_tables(chosen, slot_count, expert_count):
    row_count = chosen.shape[0]
    pick_count = chosen.shape[1]
    flat_pick = chosen.reshape(row_count * pick_count)
    hit_marks = (flat_pick[:, None] == jnp.arange(expert_count, dtype=jnp.int32)[None, :]).astype(
        jnp.int32
    )
    before = jnp.cumsum(hit_marks, axis=0) - hit_marks
    slot_place = jnp.sum(before * hit_marks, axis=1)
    target = flat_pick * slot_count + slot_place
    slot_table = target[:, None] == jnp.arange(expert_count * slot_count, dtype=jnp.int32)[None, :]
    return slot_table.astype(jnp.bfloat16).reshape(row_count, pick_count, expert_count * slot_count)


def routed_body(
    residual,
    queries_wide,
    keys_wide,
    values_wide,
    queries_narrow,
    keys_narrow,
    values_narrow,
    query_gain_wide,
    key_gain_wide,
    query_gain_narrow,
    key_gain_narrow,
    output_wide,
    output_narrow,
    norm_gain,
    gate_weight,
    up_weight,
    down_weight,
    route_ids,
    route_weights,
):
    tok_count = queries_wide.shape[0]
    places = lax.axis_index("sp") * tok_count + jnp.arange(tok_count, dtype=jnp.int32)
    wide_width = query_gain_wide.shape[0]
    narrow_width = query_gain_narrow.shape[0]
    cos_wide, sin_wide = rotary_tables(places, wide_width)
    cos_narrow, sin_narrow = rotary_tables(places, narrow_width)
    wide_keyheads = keys_wide.shape[1] // wide_width
    narrow_keyheads = keys_narrow.shape[1] // narrow_width
    q_wide = head_norm_rotate(
        queries_wide.reshape(tok_count, -1, wide_width), query_gain_wide, cos_wide, sin_wide
    )
    q_wide = q_wide.reshape(tok_count, wide_keyheads, -1, wide_width)
    k_wide = head_norm_rotate(
        keys_wide.reshape(tok_count, -1, wide_width), key_gain_wide, cos_wide, sin_wide
    )
    k_wide = k_wide.reshape(tok_count, -1)
    q_narrow = head_norm_rotate(
        queries_narrow.reshape(tok_count, -1, narrow_width),
        query_gain_narrow,
        cos_narrow,
        sin_narrow,
    )
    q_narrow = q_narrow.reshape(tok_count, narrow_keyheads, -1, narrow_width)
    k_narrow = head_norm_rotate(
        keys_narrow.reshape(tok_count, -1, narrow_width), key_gain_narrow, cos_narrow, sin_narrow
    )
    k_narrow = k_narrow.reshape(tok_count, -1)
    carried = (fresh_state(q_wide), fresh_state(q_narrow))
    carried = (
        key_sweep(
            carried[0],
            q_wide,
            lax.all_gather(k_wide, "sp", axis=0, tiled=True),
            lax.all_gather(values_wide, "sp", axis=0, tiled=True),
        ),
        key_sweep(
            carried[1],
            q_narrow,
            lax.all_gather(k_narrow, "sp", axis=0, tiled=True),
            lax.all_gather(values_narrow, "sp", axis=0, tiled=True),
        ),
    )
    heads_wide = finish_heads(carried[0])
    heads_narrow = finish_heads(carried[1])
    own_rows = residual.shape[0]
    mixed_heads = lax.psum_scatter(
        (
            jnp.dot(heads_wide, output_wide, preferred_element_type=jnp.float32)
            + jnp.dot(heads_narrow, output_narrow, preferred_element_type=jnp.float32)
        ).astype(jnp.bfloat16),
        "tp",
        scatter_dimension=0,
        tiled=True,
    ).astype(jnp.float32)
    attended = (residual.astype(jnp.float32) + mixed_heads).astype(jnp.bfloat16)
    state_float = attended.astype(jnp.float32)
    normed = (
        state_float
        * lax.rsqrt(jnp.mean(state_float * state_float, axis=-1, keepdims=True) + EPS)
        * norm_gain
    ).astype(jnp.bfloat16)
    pick_count = route_ids.shape[1]
    expert_count = lax.axis_size("sp")
    slot_count = 2 * pick_count * own_rows // expert_count
    model_width = residual.shape[1]
    own_tables = slot_tables(route_ids, slot_count, expert_count)
    send_rows = jnp.einsum(
        "rks,rd->sd", own_tables, normed, preferred_element_type=jnp.float32
    ).astype(jnp.bfloat16)
    send_rows = send_rows.reshape(expert_count, slot_count, model_width)
    arrived = lax.all_to_all(send_rows, "sp", split_axis=0, concat_axis=0, tiled=True)
    copies = lax.all_gather(arrived, "tp", axis=0, tiled=True)
    expert_arrived = copies.reshape((lax.axis_size("tp"),) + arrived.shape)
    full_shape = expert_arrived.shape
    flat_rows = expert_arrived.reshape(-1, model_width)
    gate_act = jnp.dot(flat_rows, gate_weight[0], preferred_element_type=jnp.float32)
    up_act = jnp.dot(flat_rows, up_weight[0], preferred_element_type=jnp.float32)
    hidden = (jax.nn.silu(gate_act) * up_act).astype(jnp.bfloat16)
    partial_value = jnp.dot(hidden, down_weight[0], preferred_element_type=jnp.float32).reshape(
        full_shape
    )
    summed = lax.psum_scatter(
        partial_value.astype(jnp.bfloat16), "tp", scatter_dimension=0, tiled=True
    ).astype(jnp.float32)
    results = summed.reshape(full_shape[1:]).astype(jnp.bfloat16)
    returned = lax.all_to_all(results, "sp", split_axis=0, concat_axis=0, tiled=True)
    returned_flat = returned.reshape(expert_count * slot_count, model_width)
    picked = jnp.einsum(
        "rks,sd->rkd", own_tables, returned_flat, preferred_element_type=jnp.float32
    )
    mixture = jnp.sum(route_weights[:, :, None] * picked, axis=1)
    return (state_float + mixture).astype(jnp.bfloat16)


VMEM_SPEC = pl.BlockSpec(memory_space=pltpu.VMEM)
MIB = 2**20


def on_core(kernel, results, args, flops=0, exps=0, vmem=24):
    moved = sum(a.size * a.dtype.itemsize for a in list(args) + list(results))
    return pl.pallas_call(
        kernel,
        out_shape=results,
        in_specs=[VMEM_SPEC] * len(args),
        out_specs=[VMEM_SPEC] * len(results),
        compiler_params=pltpu.CompilerParams(vmem_limit_bytes=vmem * MIB),
        cost_estimate=pl.CostEstimate(
            flops=int(flops), bytes_accessed=int(moved), transcendentals=int(exps)
        ),
    )(*args)


def like(rows, cols, dtype=jnp.bfloat16):
    return jax.ShapeDtypeStruct((rows, cols), dtype)


def lanes_of(shape):
    return lax.broadcasted_iota(jnp.int32, shape, 1)


def turned(values, quarter):
    width = values.shape[1]
    ahead = pltpu.roll(values, width - quarter, 1)
    behind = pltpu.roll(values, quarter, 1)
    return jnp.where(lanes_of(values.shape) % (2 * quarter) < quarter, ahead, behind)


def rotated(scaled, quarter, cos_table, sin_table):
    return (scaled * cos_table + turned(scaled, quarter) * sin_table).astype(jnp.bfloat16)


def rms(values, width):
    return lax.rsqrt(jnp.sum(values * values, axis=1, keepdims=True) / width + EPS)


def pack_kernel(kw_ref, vw_ref, kn_ref, vn_ref, out_ref):
    at = 0
    for ref in (kw_ref, vw_ref, kn_ref, vn_ref):
        out_ref[:, at : at + ref.shape[1]] = ref[...]
        at += ref.shape[1]


def prepare_kernel(
    order,
    own_rows,
    qw_ref,
    qn_ref,
    gw_ref,
    gn_ref,
    fw_ref,
    fn_ref,
    qw_out,
    qn_out,
    cw_ref,
    sw_ref,
    cn_ref,
    sn_ref,
):
    tokens, lanes = cw_ref.shape
    grid_rows = tokens // GRID
    for freq_ref, width, cos_ref, sin_ref in (
        (fw_ref, lanes, cw_ref, sw_ref),
        (fn_ref, lanes // 2, cn_ref, sn_ref),
    ):
        freq = freq_ref[...]
        row_at = lax.broadcasted_iota(jnp.int32, (grid_rows, lanes), 0).astype(jnp.float32) * freq
        col_at = lax.broadcasted_iota(jnp.int32, (GRID, lanes), 0).astype(jnp.float32) * freq
        quarter = width // 4
        row_cos, row_sin = jnp.cos(row_at), jnp.sin(row_at)
        col_cos, col_sin = jnp.cos(col_at), jnp.sin(col_at)
        lane = lanes_of((GRID, lanes))
        minus = lane % (2 * quarter) < quarter
        by_row = lane % width < width // 2
        for i in range(grid_rows):
            here = pl.ds(i * GRID, GRID)
            cos_ref[here, :] = jnp.where(by_row, row_cos[i : i + 1, :], col_cos)
            sines = jnp.where(by_row, row_sin[i : i + 1, :], col_sin)
            sin_ref[here, :] = jnp.where(minus, -sines, sines)
    sp, tp = lax.axis_index("sp"), lax.axis_index("tp")
    count = len(order) * own_rows
    wide = gw_ref.shape[1]
    for slot, r in enumerate(order):
        source = pl.ds(pl.multiple_of((tp ^ r) * own_rows, own_rows), own_rows)
        place = pl.ds(pl.multiple_of(sp * count + (tp ^ r) * own_rows, own_rows), own_rows)
        target = pl.ds(slot * own_rows, own_rows)
        for h in range(qw_ref.shape[1] // wide):
            head = pl.ds(h * wide, wide)
            value = qw_ref[source, head].astype(jnp.float32)
            value = value * rms(value, wide) * gw_ref[...]
            qw_out[target, head] = rotated(value, wide // 4, cw_ref[place, :], sw_ref[place, :])
        value = qn_ref[source, :].astype(jnp.float32)
        low = lanes_of(value.shape) < lanes // 2
        first = rms(jnp.where(low, value, 0.0), lanes // 2)
        second = rms(jnp.where(low, 0.0, value), lanes // 2)
        value = value * jnp.where(low, first, second) * gn_ref[...]
        qn_out[target, :] = rotated(value, lanes // 8, cn_ref[place, :], sn_ref[place, :])


def head_mix(query, keys, values, scale):
    scores = lax.dot_general(
        query, keys, (((1,), (1,)), ((), ())), preferred_element_type=jnp.float32
    )
    top = jnp.max(scores, axis=1, keepdims=True)
    weights = jnp.exp((scores - top) * scale)
    weight_sum = jnp.sum(weights, axis=1, keepdims=True)
    mixed = jnp.dot(weights.astype(jnp.bfloat16), values, preferred_element_type=jnp.float32)
    return mixed / weight_sum


def attend_kernel(
    n_sp,
    own_rows,
    *refs,
):
    raw_refs = refs[:n_sp]
    qw_ref, qn_ref, gw_ref, gn_ref, cw_ref, sw_ref, cn_ref, sn_ref, ow_ref, on_ref = refs[
        n_sp : n_sp + 10
    ]
    keep_ref, send_ref = refs[n_sp + 10 : n_sp + 12]
    count = qw_ref.shape[0]
    lanes = gw_ref.shape[1]
    sp = lax.axis_index("sp")
    kw, vw, kn, vn = [], [], [], []
    for r, ref in enumerate(raw_refs):
        place = pl.ds(pl.multiple_of((sp ^ r) * count, count), count)
        value = ref[:, :lanes].astype(jnp.float32)
        value = value * rms(value, lanes) * gw_ref[...]
        kw.append(rotated(value, lanes // 4, cw_ref[place, :], sw_ref[place, :]))
        vw.append(ref[:, lanes : 2 * lanes])
        both = ref[:, 2 * lanes :].astype(jnp.float32)
        low = lanes_of(both.shape) < lanes // 2
        other = pltpu.roll(both, lanes // 2, 1)
        value = jnp.where(low, both, other)
        value = value * rms(jnp.where(low, both, 0.0), lanes // 2) * gn_ref[...]
        kn.append(rotated(value, lanes // 8, cn_ref[place, :], sn_ref[place, :]))
        vn.append(jnp.where(low, other, both).astype(jnp.bfloat16))
    kw, vw, kn, vn = [jnp.concatenate(v, axis=0) for v in (kw, vw, kn, vn)]
    heads = []
    for h in range(qw_ref.shape[1] // lanes):
        query = qw_ref[:, h * lanes : (h + 1) * lanes]
        heads.append(head_mix(query, kw, vw, lanes**-0.5).astype(jnp.bfloat16))
    query = qn_ref[...]
    low = lanes_of(query.shape) < lanes // 2
    nothing = jnp.zeros_like(query)
    first = head_mix(jnp.where(low, query, nothing), kn, vn, (lanes // 2) ** -0.5)
    second = head_mix(jnp.where(low, nothing, query), kn, vn, (lanes // 2) ** -0.5)
    narrow = jnp.where(low, first, second).astype(jnp.bfloat16)
    wide = jnp.concatenate(heads, axis=1)
    terms = jnp.dot(wide, ow_ref[...], preferred_element_type=jnp.float32)
    terms = terms + jnp.dot(narrow, on_ref[...], preferred_element_type=jnp.float32)
    terms = terms.astype(jnp.bfloat16)
    half = terms.shape[0] // 2
    keep_ref[...] = terms[:half]
    send_ref[...] = terms[half:]


def norm_kernel(res_ref, keep_ref, came_ref, crossed_ref, gain_ref, att_ref, normed_ref):
    rows = res_ref.shape[0]
    term = keep_ref[:rows, :].astype(jnp.float32) + came_ref[:rows, :].astype(jnp.float32)
    term = term + crossed_ref[...].astype(jnp.float32)
    attended = (res_ref[...].astype(jnp.float32) + term).astype(jnp.bfloat16)
    att_ref[...] = attended
    state = attended.astype(jnp.float32)
    normed_ref[...] = (state * rms(state, state.shape[1]) * gain_ref[...]).astype(jnp.bfloat16)


def expert_kernel(r0_ref, r2_ref, r1_ref, r3_ref, gate_ref, up_ref, down_ref, keep_ref, send_ref):
    rows = jnp.concatenate([ref[...] for ref in (r0_ref, r2_ref, r1_ref, r3_ref)], axis=0)
    gate_act = jnp.dot(rows, gate_ref[0], preferred_element_type=jnp.float32)
    up_act = jnp.dot(rows, up_ref[0], preferred_element_type=jnp.float32)
    hidden = (gate_act / (1.0 + jnp.exp(-gate_act)) * up_act).astype(jnp.bfloat16)
    piece = jnp.dot(hidden, down_ref[0], preferred_element_type=jnp.float32).astype(jnp.bfloat16)
    half = piece.shape[0] // 2
    keep_ref[...] = piece[:half]
    send_ref[...] = piece[half:]


def lane_freqs(width, lanes):
    quarter = width // 4
    freq = THETA ** (-np.arange(quarter, dtype=np.float64) / quarter)
    return jnp.asarray(np.tile(freq, lanes // quarter)[None, :], jnp.float32)


def dense_body(
    residual,
    queries_wide,
    keys_wide,
    values_wide,
    queries_narrow,
    keys_narrow,
    values_narrow,
    query_gain_wide,
    key_gain_wide,
    query_gain_narrow,
    key_gain_narrow,
    output_wide,
    output_narrow,
    norm_gain,
    gate_weight,
    up_weight,
    down_weight,
    route_ids,
    route_weights,
):
    n_sp, n_tp = lax.axis_size("sp"), lax.axis_size("tp")
    sp = lax.axis_index("sp")
    tok_count, own_rows = queries_wide.shape[0], residual.shape[0]
    model_width = residual.shape[1]
    hidden_width = gate_weight.shape[2]
    lanes = query_gain_wide.shape[0]
    tokens = n_sp * tok_count
    order = [r for r in range(n_tp) if r % 2 == 0] + [r for r in range(n_tp) if r % 2]
    half = tok_count // 2

    def across(value, axis, step):
        size = lax.axis_size(axis)
        return lax.ppermute(value, axis, [(i, i ^ step) for i in range(size)])

    cut = [keys_wide, values_wide, keys_narrow, values_narrow]
    raw = on_core(pack_kernel, [like(tok_count, sum(a.shape[1] for a in cut))], cut)[0]
    raw_blocks = [raw] + [across(raw, "sp", r) for r in range(1, n_sp)]

    def twice(gain_vec):
        return jnp.concatenate([gain_vec, gain_vec])[None, :]

    table = like(tokens, lanes, jnp.float32)
    q_wide, q_narrow, *tables = on_core(
        functools.partial(prepare_kernel, order, own_rows),
        [like(*queries_wide.shape), like(*queries_narrow.shape)] + [table] * 4,
        [
            queries_wide,
            queries_narrow,
            query_gain_wide[None, :],
            twice(query_gain_narrow),
            lane_freqs(lanes, lanes),
            lane_freqs(lanes // 2, lanes),
        ],
    )
    heads = queries_wide.shape[1] // lanes + queries_narrow.shape[1] // (lanes // 2)
    keep, send = on_core(
        functools.partial(attend_kernel, n_sp, own_rows),
        [like(half, model_width)] * 2,
        raw_blocks
        + [q_wide, q_narrow, key_gain_wide[None, :], twice(key_gain_narrow)]
        + tables
        + [output_wide, output_narrow],
        flops=4 * heads * tok_count * tokens * lanes,
        exps=heads * tok_count * tokens,
        vmem=32,
    )
    came = across(send, "tp", 1)

    def crossing(keep, came):
        pair = keep[own_rows:].astype(jnp.float32) + came[own_rows:].astype(jnp.float32)
        return across(pair.astype(jnp.bfloat16), "tp", 2)

    attended, normed = on_core(
        norm_kernel,
        [like(own_rows, model_width)] * 2,
        [residual, keep, came, crossing(keep, came), norm_gain[None, :]],
    )

    total = attended.astype(jnp.float32)
    arrived = [normed] + [across(normed, "sp", r) for r in range(1, n_sp)]
    for r in range(n_sp):
        rows = [arrived[r], across(arrived[r], "tp", 2)]
        rows = rows + [across(block, "tp", 1) for block in rows]
        keep, send = on_core(
            expert_kernel,
            [like(half, model_width)] * 2,
            rows + [gate_weight, up_weight, down_weight],
            flops=6 * tok_count * model_width * hidden_width,
            exps=tok_count * hidden_width,
        )
        came = across(send, "tp", 1)
        crossed = crossing(keep, came).astype(jnp.float32)
        expert_out = keep[:own_rows].astype(jnp.float32) + came[:own_rows].astype(jnp.float32)
        expert_out = (expert_out + crossed).astype(jnp.bfloat16)
        if r:
            expert_out = across(expert_out, "sp", r)
        weight = jnp.sum(jnp.where(route_ids == (sp ^ r), route_weights, 0.0), axis=1)
        total = total + weight[:, None] * expert_out.astype(jnp.float32)
    return total.astype(jnp.bfloat16)


def body(*arrays):
    own_rows, pick_count = arrays[17].shape
    slot_count = 2 * pick_count * own_rows // lax.axis_size("sp")
    every_row_fits = slot_count >= own_rows and lax.axis_size("sp") == lax.axis_size("tp") == 4
    wide, narrow = arrays[7].shape[0], arrays[9].shape[0]
    one_key_head = arrays[2].shape[1] == wide and arrays[5].shape[1] == narrow
    full_lanes = wide == 128 and 2 * narrow == wide and arrays[4].shape[1] == wide
    whole_rows = arrays[1].shape[0] % GRID == 0 and own_rows % 8 == 0
    if every_row_fits and one_key_head and full_lanes and whole_rows:
        return dense_body(*arrays)
    return routed_body(*arrays)


def solution(mesh):
    return jax.shard_map(
        body,
        mesh=mesh,
        in_specs=(
            P(("grp", "sp", "tp"), None),
            P(("grp", "sp"), "tp"),
            P(("grp", "sp"), "tp"),
            P(("grp", "sp"), "tp"),
            P(("grp", "sp"), "tp"),
            P(("grp", "sp"), "tp"),
            P(("grp", "sp"), "tp"),
            P(),
            P(),
            P(),
            P(),
            P("tp", None),
            P("tp", None),
            P(),
            P("sp", None, "tp"),
            P("sp", None, "tp"),
            P("sp", "tp", None),
            P(("grp", "sp", "tp"), None),
            P(("grp", "sp", "tp"), None),
        ),
        out_specs=P(("grp", "sp", "tp"), None),
        check_vma=False,
    )
```

```python
import functools

import jax
import jax.numpy as jnp
import numpy as np
from jax import lax
from jax.experimental import pallas as pl
from jax.experimental.pallas import tpu as pltpu
from jax.sharding import PartitionSpec as P

GRID = 64


THETA = 10000.0
EPS = 1e-06
NEG_BIG = -1e30


def rotary_tables(places, head_width):
    quarter = head_width // 4
    inv_freq = THETA ** (-jnp.arange(quarter, dtype=jnp.float32) / quarter)
    grid_rows = (places // GRID).astype(jnp.float32)
    grid_cols = (places % GRID).astype(jnp.float32)
    row_angle = grid_rows[:, None] * inv_freq[None, :]
    col_angle = grid_cols[:, None] * inv_freq[None, :]
    angles = jnp.concatenate([row_angle, row_angle, col_angle, col_angle], axis=-1)
    return (jnp.cos(angles), jnp.sin(angles))


def head_norm_rotate(values, gain_vec, cos_table, sin_table):
    as_float = values.astype(jnp.float32)
    scaled = as_float * lax.rsqrt(jnp.mean(as_float * as_float, axis=-1, keepdims=True) + EPS)
    scaled = scaled * gain_vec
    full_shape = scaled.shape
    quarter = full_shape[-1] // 4
    halves = scaled.reshape(full_shape[:-1] + (2, 2, quarter))
    turned = jnp.stack([-halves[..., 1, :], halves[..., 0, :]], axis=-2).reshape(full_shape)
    return (scaled * cos_table[:, None, :] + turned * sin_table[:, None, :]).astype(jnp.bfloat16)


def fresh_state(queries):
    key_heads, group_size, tok_count = (queries.shape[1], queries.shape[2], queries.shape[0])
    return (
        jnp.full((key_heads, group_size, tok_count), NEG_BIG, jnp.float32),
        jnp.zeros((key_heads, group_size, tok_count), jnp.float32),
        jnp.zeros(queries.shape, jnp.float32),
    )


def key_sweep(carried, queries, keys, values):
    key_count = keys.shape[0]
    key_heads = queries.shape[1]
    head_width = queries.shape[3]
    block_len = 2048 if key_count % 2048 == 0 else key_count
    key_blocks = keys.reshape(key_count // block_len, block_len, key_heads, head_width)
    value_blocks = values.reshape(key_count // block_len, block_len, key_heads, head_width)
    score_scale = head_width ** (-0.5)

    def step(carried_state, blocks_in):
        key_block, value_block = blocks_in
        running_max, weight_sum, weighted = carried_state
        scores = (
            jnp.einsum("qhgd,khd->hgqk", queries, key_block, preferred_element_type=jnp.float32)
            * score_scale
        )
        new_max = jnp.maximum(running_max, jnp.max(scores, axis=-1))
        weights = jnp.exp(scores - new_max[..., None])
        rescale = jnp.exp(running_max - new_max)
        weight_sum = weight_sum * rescale + jnp.sum(weights, axis=-1)
        mixed_values = jnp.einsum(
            "hgqk,khd->qhgd",
            weights.astype(jnp.bfloat16),
            value_block,
            preferred_element_type=jnp.float32,
        )
        weighted = weighted * jnp.transpose(rescale, (2, 0, 1))[..., None] + mixed_values
        return ((new_max, weight_sum, weighted), None)

    carried, _ = lax.scan(step, carried, (key_blocks, value_blocks))
    return carried


def finish_heads(carried):
    weighted = carried[2]
    outcome = weighted / jnp.transpose(carried[1], (2, 0, 1))[..., None]
    return outcome.astype(jnp.bfloat16).reshape(weighted.shape[0], -1)


def slot_tables(chosen, slot_count, expert_count):
    row_count = chosen.shape[0]
    pick_count = chosen.shape[1]
    flat_pick = chosen.reshape(row_count * pick_count)
    hit_marks = (flat_pick[:, None] == jnp.arange(expert_count, dtype=jnp.int32)[None, :]).astype(
        jnp.int32
    )
    before = jnp.cumsum(hit_marks, axis=0) - hit_marks
    slot_place = jnp.sum(before * hit_marks, axis=1)
    target = flat_pick * slot_count + slot_place
    slot_table = target[:, None] == jnp.arange(expert_count * slot_count, dtype=jnp.int32)[None, :]
    return slot_table.astype(jnp.bfloat16).reshape(row_count, pick_count, expert_count * slot_count)


def routed_body(
    residual,
    queries_wide,
    keys_wide,
    values_wide,
    queries_narrow,
    keys_narrow,
    values_narrow,
    query_gain_wide,
    key_gain_wide,
    query_gain_narrow,
    key_gain_narrow,
    output_wide,
    output_narrow,
    norm_gain,
    gate_weight,
    up_weight,
    down_weight,
    route_ids,
    route_weights,
):
    tok_count = queries_wide.shape[0]
    places = lax.axis_index("sp") * tok_count + jnp.arange(tok_count, dtype=jnp.int32)
    wide_width = query_gain_wide.shape[0]
    narrow_width = query_gain_narrow.shape[0]
    cos_wide, sin_wide = rotary_tables(places, wide_width)
    cos_narrow, sin_narrow = rotary_tables(places, narrow_width)
    wide_keyheads = keys_wide.shape[1] // wide_width
    narrow_keyheads = keys_narrow.shape[1] // narrow_width
    q_wide = head_norm_rotate(
        queries_wide.reshape(tok_count, -1, wide_width), query_gain_wide, cos_wide, sin_wide
    )
    q_wide = q_wide.reshape(tok_count, wide_keyheads, -1, wide_width)
    k_wide = head_norm_rotate(
        keys_wide.reshape(tok_count, -1, wide_width), key_gain_wide, cos_wide, sin_wide
    )
    k_wide = k_wide.reshape(tok_count, -1)
    q_narrow = head_norm_rotate(
        queries_narrow.reshape(tok_count, -1, narrow_width),
        query_gain_narrow,
        cos_narrow,
        sin_narrow,
    )
    q_narrow = q_narrow.reshape(tok_count, narrow_keyheads, -1, narrow_width)
    k_narrow = head_norm_rotate(
        keys_narrow.reshape(tok_count, -1, narrow_width), key_gain_narrow, cos_narrow, sin_narrow
    )
    k_narrow = k_narrow.reshape(tok_count, -1)
    carried = (fresh_state(q_wide), fresh_state(q_narrow))
    carried = (
        key_sweep(
            carried[0],
            q_wide,
            lax.all_gather(k_wide, "sp", axis=0, tiled=True),
            lax.all_gather(values_wide, "sp", axis=0, tiled=True),
        ),
        key_sweep(
            carried[1],
            q_narrow,
            lax.all_gather(k_narrow, "sp", axis=0, tiled=True),
            lax.all_gather(values_narrow, "sp", axis=0, tiled=True),
        ),
    )
    heads_wide = finish_heads(carried[0])
    heads_narrow = finish_heads(carried[1])
    own_rows = residual.shape[0]
    mixed_heads = lax.psum_scatter(
        (
            jnp.dot(heads_wide, output_wide, preferred_element_type=jnp.float32)
            + jnp.dot(heads_narrow, output_narrow, preferred_element_type=jnp.float32)
        ).astype(jnp.bfloat16),
        "tp",
        scatter_dimension=0,
        tiled=True,
    ).astype(jnp.float32)
    attended = (residual.astype(jnp.float32) + mixed_heads).astype(jnp.bfloat16)
    state_float = attended.astype(jnp.float32)
    normed = (
        state_float
        * lax.rsqrt(jnp.mean(state_float * state_float, axis=-1, keepdims=True) + EPS)
        * norm_gain
    ).astype(jnp.bfloat16)
    pick_count = route_ids.shape[1]
    expert_count = lax.axis_size("sp")
    slot_count = 2 * pick_count * own_rows // expert_count
    model_width = residual.shape[1]
    own_tables = slot_tables(route_ids, slot_count, expert_count)
    send_rows = jnp.einsum(
        "rks,rd->sd", own_tables, normed, preferred_element_type=jnp.float32
    ).astype(jnp.bfloat16)
    send_rows = send_rows.reshape(expert_count, slot_count, model_width)
    arrived = lax.all_to_all(send_rows, "sp", split_axis=0, concat_axis=0, tiled=True)
    copies = lax.all_gather(arrived, "tp", axis=0, tiled=True)
    expert_arrived = copies.reshape((lax.axis_size("tp"),) + arrived.shape)
    full_shape = expert_arrived.shape
    flat_rows = expert_arrived.reshape(-1, model_width)
    gate_act = jnp.dot(flat_rows, gate_weight[0], preferred_element_type=jnp.float32)
    up_act = jnp.dot(flat_rows, up_weight[0], preferred_element_type=jnp.float32)
    hidden = (jax.nn.silu(gate_act) * up_act).astype(jnp.bfloat16)
    partial_value = jnp.dot(hidden, down_weight[0], preferred_element_type=jnp.float32).reshape(
        full_shape
    )
    summed = lax.psum_scatter(
        partial_value.astype(jnp.bfloat16), "tp", scatter_dimension=0, tiled=True
    ).astype(jnp.float32)
    results = summed.reshape(full_shape[1:]).astype(jnp.bfloat16)
    returned = lax.all_to_all(results, "sp", split_axis=0, concat_axis=0, tiled=True)
    returned_flat = returned.reshape(expert_count * slot_count, model_width)
    picked = jnp.einsum(
        "rks,sd->rkd", own_tables, returned_flat, preferred_element_type=jnp.float32
    )
    mixture = jnp.sum(route_weights[:, :, None] * picked, axis=1)
    return (state_float + mixture).astype(jnp.bfloat16)


VMEM_SPEC = pl.BlockSpec(memory_space=pltpu.VMEM)
MIB = 2**20
WAIT_FLOPS = 8 * 10**9


def on_core(kernel, results, args, flops=0, exps=0, vmem=24):
    moved = sum(a.size * a.dtype.itemsize for a in list(args) + list(results))
    return pl.pallas_call(
        kernel,
        out_shape=results,
        in_specs=[VMEM_SPEC] * len(args),
        out_specs=[VMEM_SPEC] * len(results),
        compiler_params=pltpu.CompilerParams(vmem_limit_bytes=vmem * MIB),
        cost_estimate=pl.CostEstimate(
            flops=int(flops), bytes_accessed=int(moved), transcendentals=int(exps)
        ),
    )(*args)


def like(rows, cols, dtype=jnp.bfloat16):
    return jax.ShapeDtypeStruct((rows, cols), dtype)


def lanes_of(shape):
    return lax.broadcasted_iota(jnp.int32, shape, 1)


def turned(values, quarter):
    width = values.shape[1]
    ahead = pltpu.roll(values, width - quarter, 1)
    behind = pltpu.roll(values, quarter, 1)
    return jnp.where(lanes_of(values.shape) % (2 * quarter) < quarter, ahead, behind)


def rotated(scaled, quarter, cos_table, sin_table):
    return (scaled * cos_table + turned(scaled, quarter) * sin_table).astype(jnp.bfloat16)


def rms(values, width):
    return lax.rsqrt(jnp.sum(values * values, axis=1, keepdims=True) / width + EPS)


def packed(wide_pair, narrow_pair):
    return jnp.concatenate(
        [jnp.concatenate(wide_pair, axis=1)] + [a.T for a in narrow_pair], axis=0
    )


def prepare_kernel(
    order,
    own_rows,
    qw_ref,
    qn_ref,
    small_ref,
    qw_out,
    qn_out,
    cw_ref,
    sw_ref,
    cn_ref,
    sn_ref,
):
    tokens, lanes = cw_ref.shape
    grid_rows = tokens // GRID
    for freq, width, cos_ref, sin_ref in (
        (small_ref[4:5, :], lanes, cw_ref, sw_ref),
        (small_ref[5:6, :], lanes // 2, cn_ref, sn_ref),
    ):
        row_at = lax.broadcasted_iota(jnp.int32, (grid_rows, lanes), 0).astype(jnp.float32) * freq
        col_at = lax.broadcasted_iota(jnp.int32, (GRID, lanes), 0).astype(jnp.float32) * freq
        quarter = width // 4
        row_cos, row_sin = jnp.cos(row_at), jnp.sin(row_at)
        col_cos, col_sin = jnp.cos(col_at), jnp.sin(col_at)
        lane = lanes_of((GRID, lanes))
        minus = lane % (2 * quarter) < quarter
        by_row = lane % width < width // 2
        for i in range(grid_rows):
            here = pl.ds(i * GRID, GRID)
            cos_ref[here, :] = jnp.where(by_row, row_cos[i : i + 1, :], col_cos)
            sines = jnp.where(by_row, row_sin[i : i + 1, :], col_sin)
            sin_ref[here, :] = jnp.where(minus, -sines, sines)
    sp, tp = lax.axis_index("sp"), lax.axis_index("tp")
    count = len(order) * own_rows
    gain_wide, gain_narrow = small_ref[0:1, :], small_ref[1:2, :]
    for slot, r in enumerate(order):
        source = pl.ds(pl.multiple_of((tp ^ r) * own_rows, own_rows), own_rows)
        place = pl.ds(pl.multiple_of(sp * count + (tp ^ r) * own_rows, own_rows), own_rows)
        target = pl.ds(slot * own_rows, own_rows)
        for h in range(qw_ref.shape[1] // lanes):
            head = pl.ds(h * lanes, lanes)
            value = qw_ref[source, head].astype(jnp.float32)
            value = value * rms(value, lanes) * gain_wide
            qw_out[target, head] = rotated(value, lanes // 4, cw_ref[place, :], sw_ref[place, :])
        value = qn_ref[source, :].astype(jnp.float32)
        low = lanes_of(value.shape) < lanes // 2
        first = rms(jnp.where(low, value, 0.0), lanes // 2)
        second = rms(jnp.where(low, 0.0, value), lanes // 2)
        value = value * jnp.where(low, first, second) * gain_narrow
        qn_out[target, :] = rotated(value, lanes // 8, cn_ref[place, :], sn_ref[place, :])


def mixed_in(query, keys, values, scale, before=None):
    scores = lax.dot_general(
        query, keys, (((1,), (1,)), ((), ())), preferred_element_type=jnp.float32
    )
    top = jnp.max(scores, axis=1, keepdims=True)
    if before is not None:
        top = jnp.maximum(top, before[0])
    weights = jnp.exp((scores - top) * scale)
    total = jnp.sum(weights, axis=1, keepdims=True)
    mixed = jnp.dot(weights.astype(jnp.bfloat16), values, preferred_element_type=jnp.float32)
    if before is not None:
        fade = jnp.exp((before[0] - top) * scale)
        total = total + before[1] * fade
        mixed = mixed + before[2] * fade
    return top, total, mixed


def keys_and_values(raw_refs, steps, small_ref, tables):
    cw_ref, sw_ref, cn_ref, sn_ref = tables
    lanes = small_ref.shape[1]
    sp = lax.axis_index("sp")
    kw, vw, kn, vn = [], [], [], []
    for r, ref in zip(steps, raw_refs, strict=True):
        count = ref.shape[0] - lanes
        place = pl.ds(pl.multiple_of((sp ^ r) * count, count), count)
        value = ref[:count, :lanes].astype(jnp.float32)
        value = value * rms(value, lanes) * small_ref[2:3, :]
        kw.append(rotated(value, lanes // 4, cw_ref[place, :], sw_ref[place, :]))
        vw.append(ref[:count, lanes:])
        both = ref[count:, :].astype(jnp.float32).T
        low = lanes_of(both.shape) < lanes // 2
        other = pltpu.roll(both, lanes // 2, 1)
        value = jnp.where(low, both, other)
        value = value * rms(jnp.where(low, both, 0.0), lanes // 2) * small_ref[3:4, :]
        kn.append(rotated(value, lanes // 8, cn_ref[place, :], sn_ref[place, :]))
        vn.append(jnp.where(low, other, both).astype(jnp.bfloat16))
    return [jnp.concatenate(v, axis=0) for v in (kw, vw, kn, vn)]


def all_heads(qw_ref, qn_ref, keys, lanes, before=None):
    kw, vw, kn, vn = keys
    query = qn_ref[...]
    low = lanes_of(query.shape) < lanes // 2
    nothing = jnp.zeros_like(query)
    heads = [
        (qw_ref[:, h * lanes : (h + 1) * lanes], kw, vw, lanes**-0.5)
        for h in range(qw_ref.shape[1] // lanes)
    ]
    heads.append((jnp.where(low, query, nothing), kn, vn, (lanes // 2) ** -0.5))
    heads.append((jnp.where(low, nothing, query), kn, vn, (lanes // 2) ** -0.5))
    before = [None] * len(heads) if before is None else before
    return [mixed_in(*head, old) for head, old in zip(heads, before, strict=True)]


def attend_first_kernel(steps, *refs):
    raw_refs, refs = refs[: len(steps)], refs[len(steps) :]
    qw_ref, qn_ref, small_ref = refs[:3]
    stat_ref, mixed_ref = refs[7:]
    lanes = small_ref.shape[1]
    keys = keys_and_values(raw_refs, steps, small_ref, refs[3:7])
    states = all_heads(qw_ref, qn_ref, keys, lanes)
    lane = lanes_of(stat_ref.shape)
    stat = jnp.zeros(stat_ref.shape, jnp.float32)
    for h, (top, total, mixed) in enumerate(states):
        stat = jnp.where(lane == 2 * h, top, stat)
        stat = jnp.where(lane == 2 * h + 1, total, stat)
        mixed_ref[h] = mixed
    stat_ref[...] = stat


def attend_last_kernel(steps, *refs):
    raw_refs, refs = refs[: len(steps)], refs[len(steps) :]
    qw_ref, qn_ref, small_ref = refs[:3]
    stat_ref, mixed_ref, ow_ref, on_ref, keep_ref, send_ref = refs[7:]
    lanes = small_ref.shape[1]
    keys = keys_and_values(raw_refs, steps, small_ref, refs[3:7])
    before = [
        (stat_ref[:, 2 * h : 2 * h + 1], stat_ref[:, 2 * h + 1 : 2 * h + 2], mixed_ref[h])
        for h in range(mixed_ref.shape[0])
    ]
    states = all_heads(qw_ref, qn_ref, keys, lanes, before)
    heads = [mixed / total for _, total, mixed in states]
    low = lanes_of(heads[-1].shape) < lanes // 2
    narrow = jnp.where(low, heads[-2], heads[-1]).astype(jnp.bfloat16)
    wide = jnp.concatenate(heads[:-2], axis=1).astype(jnp.bfloat16)
    terms = jnp.dot(wide, ow_ref[...], preferred_element_type=jnp.float32)
    terms = terms + jnp.dot(narrow, on_ref[...], preferred_element_type=jnp.float32)
    terms = terms.astype(jnp.bfloat16)
    half = terms.shape[0] // 2
    keep_ref[...] = terms[:half]
    send_ref[...] = terms[half:]


def norm_kernel(res_ref, keep_ref, came_ref, crossed_ref, gain_ref, att_ref, normed_ref):
    rows = res_ref.shape[0]
    term = keep_ref[:rows, :].astype(jnp.float32) + came_ref[:rows, :].astype(jnp.float32)
    term = term + crossed_ref[...].astype(jnp.float32)
    attended = (res_ref[...].astype(jnp.float32) + term).astype(jnp.bfloat16)
    att_ref[...] = attended
    state = attended.astype(jnp.float32)
    normed_ref[...] = (state * rms(state, state.shape[1]) * gain_ref[...]).astype(jnp.bfloat16)


def expert_kernel(r0_ref, r2_ref, r1_ref, r3_ref, gate_ref, up_ref, down_ref, keep_ref, send_ref):
    rows = jnp.concatenate([ref[...] for ref in (r0_ref, r2_ref, r1_ref, r3_ref)], axis=0)
    gate_act = jnp.dot(rows, gate_ref[0], preferred_element_type=jnp.float32)
    up_act = jnp.dot(rows, up_ref[0], preferred_element_type=jnp.float32)
    hidden = (gate_act / (1.0 + jnp.exp(-gate_act)) * up_act).astype(jnp.bfloat16)
    piece = jnp.dot(hidden, down_ref[0], preferred_element_type=jnp.float32).astype(jnp.bfloat16)
    half = piece.shape[0] // 2
    keep_ref[...] = piece[:half]
    send_ref[...] = piece[half:]


def lane_freqs(width, lanes):
    quarter = width // 4
    freq = THETA ** (-np.arange(quarter, dtype=np.float64) / quarter)
    return jnp.asarray(np.tile(freq, lanes // quarter), jnp.float32)


def dense_body(
    residual,
    queries_wide,
    keys_wide,
    values_wide,
    queries_narrow,
    keys_narrow,
    values_narrow,
    query_gain_wide,
    key_gain_wide,
    query_gain_narrow,
    key_gain_narrow,
    output_wide,
    output_narrow,
    norm_gain,
    gate_weight,
    up_weight,
    down_weight,
    route_ids,
    route_weights,
):
    n_sp, n_tp = lax.axis_size("sp"), lax.axis_size("tp")
    sp = lax.axis_index("sp")
    tok_count, own_rows = queries_wide.shape[0], residual.shape[0]
    model_width = residual.shape[1]
    hidden_width = gate_weight.shape[2]
    lanes = query_gain_wide.shape[0]
    tokens = n_sp * tok_count
    order = [r for r in range(n_tp) if r % 2 == 0] + [r for r in range(n_tp) if r % 2]
    half = tok_count // 2

    def across(value, axis, step):
        size = lax.axis_size(axis)
        return lax.ppermute(value, axis, [(i, i ^ step) for i in range(size)])

    def spread(own):
        two = across(own, "sp", 2)
        one = across(own, "sp", 1)
        return [own, one, two, across(two, "sp", 1)]

    raw_blocks = spread(packed([keys_wide, values_wide], [keys_narrow, values_narrow]))

    table = like(tokens, lanes, jnp.float32)
    small = jnp.concatenate(
        [query_gain_wide, query_gain_narrow, query_gain_narrow]
        + [key_gain_wide, key_gain_narrow, key_gain_narrow]
        + [lane_freqs(lanes, lanes), lane_freqs(lanes // 2, lanes)]
    ).reshape(6, lanes)
    q_wide, q_narrow, *tables = on_core(
        functools.partial(prepare_kernel, order, own_rows),
        [like(*queries_wide.shape), like(*queries_narrow.shape)] + [table] * 4,
        [queries_wide, queries_narrow, small],
        flops=WAIT_FLOPS,
    )
    heads = queries_wide.shape[1] // lanes + queries_narrow.shape[1] // (lanes // 2)
    shared = [q_wide, q_narrow, small] + tables
    one_block = dict(flops=WAIT_FLOPS, exps=heads * tok_count**2)
    stat, mixed = on_core(
        functools.partial(attend_first_kernel, (0, 1, 2)),
        [
            like(tok_count, lanes, jnp.float32),
            jax.ShapeDtypeStruct((heads, tok_count, lanes), jnp.float32),
        ],
        raw_blocks[:3] + shared,
        **one_block,
    )
    keep, send = on_core(
        functools.partial(attend_last_kernel, (3,)),
        [like(half, model_width)] * 2,
        raw_blocks[3:] + shared + [stat, mixed, output_wide, output_narrow],
        **one_block,
    )
    came = across(send, "tp", 1)

    def crossing(keep, came):
        pair = keep[own_rows:].astype(jnp.float32) + came[own_rows:].astype(jnp.float32)
        return across(pair.astype(jnp.bfloat16), "tp", 2)

    attended, normed = on_core(
        norm_kernel,
        [like(own_rows, model_width)] * 2,
        [residual, keep, came, crossing(keep, came), norm_gain[None, :]],
    )

    total = attended.astype(jnp.float32)
    arrived = spread(normed)
    crossed_rows = []
    for r in range(n_sp):
        if r % 2:
            crossed_rows.append(across(crossed_rows[r - 1], "sp", 1))
        else:
            crossed_rows.append(across(arrived[r], "tp", 2))
        rows = [arrived[r], crossed_rows[r]]
        rows = rows + [across(rows[0], "tp", 1), across(rows[1], "tp", 1)]
        keep, send = on_core(
            expert_kernel,
            [like(half, model_width)] * 2,
            rows + [gate_weight, up_weight, down_weight],
            flops=6 * tok_count * model_width * hidden_width,
            exps=tok_count * hidden_width,
        )
        came = across(send, "tp", 1)
        crossed = crossing(keep, came).astype(jnp.float32)
        expert_out = keep[:own_rows].astype(jnp.float32) + came[:own_rows].astype(jnp.float32)
        expert_out = (expert_out + crossed).astype(jnp.bfloat16)
        if r:
            expert_out = across(expert_out, "sp", r)
        weight = jnp.sum(jnp.where(route_ids == (sp ^ r), route_weights, 0.0), axis=1)
        total = total + weight[:, None] * expert_out.astype(jnp.float32)
    return total.astype(jnp.bfloat16)


def body(*arrays):
    own_rows, pick_count = arrays[17].shape
    slot_count = 2 * pick_count * own_rows // lax.axis_size("sp")
    every_row_fits = slot_count >= own_rows and lax.axis_size("sp") == lax.axis_size("tp") == 4
    wide, narrow = arrays[7].shape[0], arrays[9].shape[0]
    one_key_head = arrays[2].shape[1] == wide and arrays[5].shape[1] == narrow
    full_lanes = wide == 128 and 2 * narrow == wide and arrays[4].shape[1] == wide
    whole_rows = arrays[1].shape[0] % GRID == 0 and own_rows % 8 == 0
    if every_row_fits and one_key_head and full_lanes and whole_rows:
        return dense_body(*arrays)
    return routed_body(*arrays)


def solution(mesh):
    return jax.shard_map(
        body,
        mesh=mesh,
        in_specs=(
            P(("grp", "sp", "tp"), None),
            P(("grp", "sp"), "tp"),
            P(("grp", "sp"), "tp"),
            P(("grp", "sp"), "tp"),
            P(("grp", "sp"), "tp"),
            P(("grp", "sp"), "tp"),
            P(("grp", "sp"), "tp"),
            P(),
            P(),
            P(),
            P(),
            P("tp", None),
            P("tp", None),
            P(),
            P("sp", None, "tp"),
            P("sp", None, "tp"),
            P("sp", "tp", None),
            P(("grp", "sp", "tp"), None),
            P(("grp", "sp", "tp"), None),
        ),
        out_specs=P(("grp", "sp", "tp"), None),
        check_vma=False,
    )
```

```python
import functools

import jax
import jax.numpy as jnp
import numpy as np
from jax import lax
from jax.experimental import pallas as pl
from jax.experimental.pallas import tpu as pltpu
from jax.sharding import PartitionSpec as P

GRID = 64


THETA = 10000.0
EPS = 1e-06
NEG_BIG = -1e30


def rotary_tables(places, head_width):
    quarter = head_width // 4
    inv_freq = THETA ** (-jnp.arange(quarter, dtype=jnp.float32) / quarter)
    grid_rows = (places // GRID).astype(jnp.float32)
    grid_cols = (places % GRID).astype(jnp.float32)
    row_angle = grid_rows[:, None] * inv_freq[None, :]
    col_angle = grid_cols[:, None] * inv_freq[None, :]
    angles = jnp.concatenate([row_angle, row_angle, col_angle, col_angle], axis=-1)
    return (jnp.cos(angles), jnp.sin(angles))


def head_norm_rotate(values, gain_vec, cos_table, sin_table):
    as_float = values.astype(jnp.float32)
    scaled = as_float * lax.rsqrt(jnp.mean(as_float * as_float, axis=-1, keepdims=True) + EPS)
    scaled = scaled * gain_vec
    full_shape = scaled.shape
    quarter = full_shape[-1] // 4
    halves = scaled.reshape(full_shape[:-1] + (2, 2, quarter))
    turned = jnp.stack([-halves[..., 1, :], halves[..., 0, :]], axis=-2).reshape(full_shape)
    return (scaled * cos_table[:, None, :] + turned * sin_table[:, None, :]).astype(jnp.bfloat16)


def fresh_state(queries):
    key_heads, group_size, tok_count = (queries.shape[1], queries.shape[2], queries.shape[0])
    return (
        jnp.full((key_heads, group_size, tok_count), NEG_BIG, jnp.float32),
        jnp.zeros((key_heads, group_size, tok_count), jnp.float32),
        jnp.zeros(queries.shape, jnp.float32),
    )


def key_sweep(carried, queries, keys, values):
    key_count = keys.shape[0]
    key_heads = queries.shape[1]
    head_width = queries.shape[3]
    block_len = 2048 if key_count % 2048 == 0 else key_count
    key_blocks = keys.reshape(key_count // block_len, block_len, key_heads, head_width)
    value_blocks = values.reshape(key_count // block_len, block_len, key_heads, head_width)
    score_scale = head_width ** (-0.5)

    def step(carried_state, blocks_in):
        key_block, value_block = blocks_in
        running_max, weight_sum, weighted = carried_state
        scores = (
            jnp.einsum("qhgd,khd->hgqk", queries, key_block, preferred_element_type=jnp.float32)
            * score_scale
        )
        new_max = jnp.maximum(running_max, jnp.max(scores, axis=-1))
        weights = jnp.exp(scores - new_max[..., None])
        rescale = jnp.exp(running_max - new_max)
        weight_sum = weight_sum * rescale + jnp.sum(weights, axis=-1)
        mixed_values = jnp.einsum(
            "hgqk,khd->qhgd",
            weights.astype(jnp.bfloat16),
            value_block,
            preferred_element_type=jnp.float32,
        )
        weighted = weighted * jnp.transpose(rescale, (2, 0, 1))[..., None] + mixed_values
        return ((new_max, weight_sum, weighted), None)

    carried, _ = lax.scan(step, carried, (key_blocks, value_blocks))
    return carried


def finish_heads(carried):
    weighted = carried[2]
    outcome = weighted / jnp.transpose(carried[1], (2, 0, 1))[..., None]
    return outcome.astype(jnp.bfloat16).reshape(weighted.shape[0], -1)


def slot_tables(chosen, slot_count, expert_count):
    row_count = chosen.shape[0]
    pick_count = chosen.shape[1]
    flat_pick = chosen.reshape(row_count * pick_count)
    hit_marks = (flat_pick[:, None] == jnp.arange(expert_count, dtype=jnp.int32)[None, :]).astype(
        jnp.int32
    )
    before = jnp.cumsum(hit_marks, axis=0) - hit_marks
    slot_place = jnp.sum(before * hit_marks, axis=1)
    target = flat_pick * slot_count + slot_place
    slot_table = target[:, None] == jnp.arange(expert_count * slot_count, dtype=jnp.int32)[None, :]
    return slot_table.astype(jnp.bfloat16).reshape(row_count, pick_count, expert_count * slot_count)


def routed_body(
    residual,
    queries_wide,
    keys_wide,
    values_wide,
    queries_narrow,
    keys_narrow,
    values_narrow,
    query_gain_wide,
    key_gain_wide,
    query_gain_narrow,
    key_gain_narrow,
    output_wide,
    output_narrow,
    norm_gain,
    gate_weight,
    up_weight,
    down_weight,
    route_ids,
    route_weights,
):
    tok_count = queries_wide.shape[0]
    places = lax.axis_index("sp") * tok_count + jnp.arange(tok_count, dtype=jnp.int32)
    wide_width = query_gain_wide.shape[0]
    narrow_width = query_gain_narrow.shape[0]
    cos_wide, sin_wide = rotary_tables(places, wide_width)
    cos_narrow, sin_narrow = rotary_tables(places, narrow_width)
    wide_keyheads = keys_wide.shape[1] // wide_width
    narrow_keyheads = keys_narrow.shape[1] // narrow_width
    q_wide = head_norm_rotate(
        queries_wide.reshape(tok_count, -1, wide_width), query_gain_wide, cos_wide, sin_wide
    )
    q_wide = q_wide.reshape(tok_count, wide_keyheads, -1, wide_width)
    k_wide = head_norm_rotate(
        keys_wide.reshape(tok_count, -1, wide_width), key_gain_wide, cos_wide, sin_wide
    )
    k_wide = k_wide.reshape(tok_count, -1)
    q_narrow = head_norm_rotate(
        queries_narrow.reshape(tok_count, -1, narrow_width),
        query_gain_narrow,
        cos_narrow,
        sin_narrow,
    )
    q_narrow = q_narrow.reshape(tok_count, narrow_keyheads, -1, narrow_width)
    k_narrow = head_norm_rotate(
        keys_narrow.reshape(tok_count, -1, narrow_width), key_gain_narrow, cos_narrow, sin_narrow
    )
    k_narrow = k_narrow.reshape(tok_count, -1)
    carried = (fresh_state(q_wide), fresh_state(q_narrow))
    carried = (
        key_sweep(
            carried[0],
            q_wide,
            lax.all_gather(k_wide, "sp", axis=0, tiled=True),
            lax.all_gather(values_wide, "sp", axis=0, tiled=True),
        ),
        key_sweep(
            carried[1],
            q_narrow,
            lax.all_gather(k_narrow, "sp", axis=0, tiled=True),
            lax.all_gather(values_narrow, "sp", axis=0, tiled=True),
        ),
    )
    heads_wide = finish_heads(carried[0])
    heads_narrow = finish_heads(carried[1])
    own_rows = residual.shape[0]
    mixed_heads = lax.psum_scatter(
        (
            jnp.dot(heads_wide, output_wide, preferred_element_type=jnp.float32)
            + jnp.dot(heads_narrow, output_narrow, preferred_element_type=jnp.float32)
        ).astype(jnp.bfloat16),
        "tp",
        scatter_dimension=0,
        tiled=True,
    ).astype(jnp.float32)
    attended = (residual.astype(jnp.float32) + mixed_heads).astype(jnp.bfloat16)
    state_float = attended.astype(jnp.float32)
    normed = (
        state_float
        * lax.rsqrt(jnp.mean(state_float * state_float, axis=-1, keepdims=True) + EPS)
        * norm_gain
    ).astype(jnp.bfloat16)
    pick_count = route_ids.shape[1]
    expert_count = lax.axis_size("sp")
    slot_count = 2 * pick_count * own_rows // expert_count
    model_width = residual.shape[1]
    own_tables = slot_tables(route_ids, slot_count, expert_count)
    send_rows = jnp.einsum(
        "rks,rd->sd", own_tables, normed, preferred_element_type=jnp.float32
    ).astype(jnp.bfloat16)
    send_rows = send_rows.reshape(expert_count, slot_count, model_width)
    arrived = lax.all_to_all(send_rows, "sp", split_axis=0, concat_axis=0, tiled=True)
    copies = lax.all_gather(arrived, "tp", axis=0, tiled=True)
    expert_arrived = copies.reshape((lax.axis_size("tp"),) + arrived.shape)
    full_shape = expert_arrived.shape
    flat_rows = expert_arrived.reshape(-1, model_width)
    gate_act = jnp.dot(flat_rows, gate_weight[0], preferred_element_type=jnp.float32)
    up_act = jnp.dot(flat_rows, up_weight[0], preferred_element_type=jnp.float32)
    hidden = (jax.nn.silu(gate_act) * up_act).astype(jnp.bfloat16)
    partial_value = jnp.dot(hidden, down_weight[0], preferred_element_type=jnp.float32).reshape(
        full_shape
    )
    summed = lax.psum_scatter(
        partial_value.astype(jnp.bfloat16), "tp", scatter_dimension=0, tiled=True
    ).astype(jnp.float32)
    results = summed.reshape(full_shape[1:]).astype(jnp.bfloat16)
    returned = lax.all_to_all(results, "sp", split_axis=0, concat_axis=0, tiled=True)
    returned_flat = returned.reshape(expert_count * slot_count, model_width)
    picked = jnp.einsum(
        "rks,sd->rkd", own_tables, returned_flat, preferred_element_type=jnp.float32
    )
    mixture = jnp.sum(route_weights[:, :, None] * picked, axis=1)
    return (state_float + mixture).astype(jnp.bfloat16)


VMEM_SPEC = pl.BlockSpec(memory_space=pltpu.VMEM)
MIB = 2**20
WAIT_FLOPS = 8 * 10**9


def on_core(kernel, results, args, flops=0, exps=0, vmem=16):
    moved = sum(a.size * a.dtype.itemsize for a in list(args) + list(results))
    return pl.pallas_call(
        kernel,
        out_shape=results,
        in_specs=[VMEM_SPEC] * len(args),
        out_specs=[VMEM_SPEC] * len(results),
        compiler_params=pltpu.CompilerParams(vmem_limit_bytes=vmem * MIB),
        cost_estimate=pl.CostEstimate(
            flops=int(flops), bytes_accessed=int(moved), transcendentals=int(exps)
        ),
    )(*args)


def like(rows, cols, dtype=jnp.bfloat16):
    return jax.ShapeDtypeStruct((rows, cols), dtype)


def lanes_of(shape):
    return lax.broadcasted_iota(jnp.int32, shape, 1)


def turned(values, quarter):
    width = values.shape[1]
    ahead = pltpu.roll(values, width - quarter, 1)
    behind = pltpu.roll(values, quarter, 1)
    return jnp.where(lanes_of(values.shape) % (2 * quarter) < quarter, ahead, behind)


def rotated(scaled, quarter, cos_table, sin_table):
    return (scaled * cos_table + turned(scaled, quarter) * sin_table).astype(jnp.bfloat16)


def rms(values, width):
    return lax.rsqrt(jnp.sum(values * values, axis=1, keepdims=True) / width + EPS)


def prepare_kernel(
    order,
    own_rows,
    query_ref,
    small_ref,
    qw_out,
    qn_out,
    cw_ref,
    sw_ref,
    cn_ref,
    sn_ref,
):
    tokens, lanes = cw_ref.shape
    grid_rows = tokens // GRID
    for freq, width, cos_ref, sin_ref in (
        (small_ref[4:5, :], lanes, cw_ref, sw_ref),
        (small_ref[5:6, :], lanes // 2, cn_ref, sn_ref),
    ):
        row_at = lax.broadcasted_iota(jnp.int32, (grid_rows, lanes), 0).astype(jnp.float32) * freq
        col_at = lax.broadcasted_iota(jnp.int32, (GRID, lanes), 0).astype(jnp.float32) * freq
        quarter = width // 4
        row_cos, row_sin = jnp.cos(row_at), jnp.sin(row_at)
        col_cos, col_sin = jnp.cos(col_at), jnp.sin(col_at)
        lane = lanes_of((GRID, lanes))
        minus = lane % (2 * quarter) < quarter
        by_row = lane % width < width // 2
        for i in range(grid_rows):
            here = pl.ds(i * GRID, GRID)
            cos_ref[here, :] = jnp.where(by_row, row_cos[i : i + 1, :], col_cos)
            sines = jnp.where(by_row, row_sin[i : i + 1, :], col_sin)
            sin_ref[here, :] = jnp.where(minus, -sines, sines)
    sp, tp = lax.axis_index("sp"), lax.axis_index("tp")
    count = len(order) * own_rows
    gain_wide, gain_narrow = small_ref[0:1, :], small_ref[1:2, :]
    for slot, r in enumerate(order):
        source = pl.ds(pl.multiple_of((tp ^ r) * own_rows, own_rows), own_rows)
        place = pl.ds(pl.multiple_of(sp * count + (tp ^ r) * own_rows, own_rows), own_rows)
        target = pl.ds(slot * own_rows, own_rows)
        for h in range(qw_out.shape[1] // lanes):
            head = pl.ds(h * lanes, lanes)
            value = query_ref[source, head].astype(jnp.float32)
            value = value * rms(value, lanes) * gain_wide
            qw_out[target, head] = rotated(value, lanes // 4, cw_ref[place, :], sw_ref[place, :])
        value = query_ref[source, qw_out.shape[1] :].astype(jnp.float32)
        low = lanes_of(value.shape) < lanes // 2
        first = rms(jnp.where(low, value, 0.0), lanes // 2)
        second = rms(jnp.where(low, 0.0, value), lanes // 2)
        value = value * jnp.where(low, first, second) * gain_narrow
        qn_out[target, :] = rotated(value, lanes // 8, cn_ref[place, :], sn_ref[place, :])


def mixed_in(query, keys, values, scale, before=None):
    scores = lax.dot_general(
        query, keys, (((1,), (1,)), ((), ())), preferred_element_type=jnp.float32
    )
    top = jnp.max(scores, axis=1, keepdims=True)
    if before is not None:
        top = jnp.maximum(top, before[0])
    weights = jnp.exp((scores - top) * scale)
    total = jnp.sum(weights, axis=1, keepdims=True)
    mixed = jnp.dot(weights.astype(jnp.bfloat16), values, preferred_element_type=jnp.float32)
    if before is not None:
        fade = jnp.exp((before[0] - top) * scale)
        total = total + before[1] * fade
        mixed = mixed + before[2] * fade
    return top, total, mixed


def wide_keys(raw_refs, steps, small_ref, cos_ref, sin_ref):
    lanes = small_ref.shape[1]
    sp = lax.axis_index("sp")
    keys, values = [], []
    for r, ref in zip(steps, raw_refs, strict=True):
        count = ref.shape[0] // 2
        place = pl.ds(pl.multiple_of((sp ^ r) * count, count), count)
        value = ref[:count, :].astype(jnp.float32)
        value = value * rms(value, lanes) * small_ref[2:3, :]
        keys.append(rotated(value, lanes // 4, cos_ref[place, :], sin_ref[place, :]))
        values.append(ref[count:, :])
    return jnp.concatenate(keys, axis=0), jnp.concatenate(values, axis=0)


def narrow_keys(raw_refs, steps, small_ref, cos_ref, sin_ref):
    lanes = small_ref.shape[1]
    sp = lax.axis_index("sp")
    keys, values = [], []
    for r, ref in zip(steps, raw_refs, strict=True):
        count = ref.shape[1]
        place = pl.ds(pl.multiple_of((sp ^ r) * count, count), count)
        both = ref[...].astype(jnp.float32).T
        low = lanes_of(both.shape) < lanes // 2
        other = pltpu.roll(both, lanes // 2, 1)
        value = jnp.where(low, both, other)
        value = value * rms(jnp.where(low, both, 0.0), lanes // 2) * small_ref[3:4, :]
        keys.append(rotated(value, lanes // 8, cos_ref[place, :], sin_ref[place, :]))
        values.append(jnp.where(low, other, both).astype(jnp.bfloat16))
    return jnp.concatenate(keys, axis=0), jnp.concatenate(values, axis=0)


def wide_queries(ref, lanes):
    return [ref[:, h * lanes : (h + 1) * lanes] for h in range(ref.shape[1] // lanes)]


def narrow_queries(ref, lanes):
    query = ref[...]
    low = lanes_of(query.shape) < lanes // 2
    nothing = jnp.zeros_like(query)
    return [jnp.where(low, query, nothing), jnp.where(low, nothing, query)]


WIDE = (wide_keys, wide_queries, 1)
NARROW = (narrow_keys, narrow_queries, 2)


def attend_first_kernel(kind, steps, *refs):
    raw_refs, refs = refs[: len(steps)], refs[len(steps) :]
    query_ref, small_ref, cos_ref, sin_ref, stat_ref, mixed_ref = refs
    lanes = small_ref.shape[1]
    keys, values = kind[0](raw_refs, steps, small_ref, cos_ref, sin_ref)
    scale = (lanes // kind[2]) ** -0.5
    lane = lanes_of(stat_ref.shape)
    stat = jnp.zeros(stat_ref.shape, jnp.float32)
    for h, query in enumerate(kind[1](query_ref, lanes)):
        top, total, mixed = mixed_in(query, keys, values, scale)
        stat = jnp.where(lane == 2 * h, top, stat)
        stat = jnp.where(lane == 2 * h + 1, total, stat)
        mixed_ref[h] = mixed
    stat_ref[...] = stat


def attend_last_kernel(kind, steps, *refs):
    raw_refs, refs = refs[: len(steps)], refs[len(steps) :]
    query_ref, small_ref, cos_ref, sin_ref, stat_ref, mixed_ref, proj_ref, *refs = refs
    lanes = small_ref.shape[1]
    keys, values = kind[0](raw_refs, steps, small_ref, cos_ref, sin_ref)
    scale = (lanes // kind[2]) ** -0.5
    heads = []
    for h, query in enumerate(kind[1](query_ref, lanes)):
        before = (stat_ref[:, 2 * h : 2 * h + 1], stat_ref[:, 2 * h + 1 : 2 * h + 2], mixed_ref[h])
        _, total, mixed = mixed_in(query, keys, values, scale, before)
        heads.append(mixed / total)
    if kind[2] == 1:
        joined = jnp.concatenate(heads, axis=1)
    else:
        joined = jnp.where(lanes_of(heads[0].shape) < lanes // 2, heads[0], heads[1])
    terms = jnp.dot(joined.astype(jnp.bfloat16), proj_ref[...], preferred_element_type=jnp.float32)
    if len(refs) == 1:
        refs[0][...] = terms
        return
    terms_ref, keep_ref, send_ref = refs
    terms = (terms_ref[...] + terms).astype(jnp.bfloat16)
    half = terms.shape[0] // 2
    keep_ref[...] = terms[:half]
    send_ref[...] = terms[half:]


def norm_kernel(res_ref, keep_ref, came_ref, crossed_ref, gain_ref, att_ref, normed_ref):
    rows = res_ref.shape[0]
    term = keep_ref[:rows, :].astype(jnp.float32) + came_ref[:rows, :].astype(jnp.float32)
    term = term + crossed_ref[...].astype(jnp.float32)
    attended = (res_ref[...].astype(jnp.float32) + term).astype(jnp.bfloat16)
    att_ref[...] = attended
    state = attended.astype(jnp.float32)
    normed_ref[...] = (state * rms(state, state.shape[1]) * gain_ref[...]).astype(jnp.bfloat16)


def expert_kernel(r0_ref, r2_ref, r1_ref, r3_ref, gate_ref, up_ref, down_ref, keep_ref, send_ref):
    rows = jnp.concatenate([ref[...] for ref in (r0_ref, r2_ref, r1_ref, r3_ref)], axis=0)
    gate_act = jnp.dot(rows, gate_ref[0], preferred_element_type=jnp.float32)
    up_act = jnp.dot(rows, up_ref[0], preferred_element_type=jnp.float32)
    hidden = (gate_act / (1.0 + jnp.exp(-gate_act)) * up_act).astype(jnp.bfloat16)
    piece = jnp.dot(hidden, down_ref[0], preferred_element_type=jnp.float32).astype(jnp.bfloat16)
    half = piece.shape[0] // 2
    keep_ref[...] = piece[:half]
    send_ref[...] = piece[half:]


def lane_freqs(width, lanes):
    quarter = width // 4
    freq = THETA ** (-np.arange(quarter, dtype=np.float64) / quarter)
    return jnp.asarray(np.tile(freq, lanes // quarter), jnp.float32)


def dense_body(
    residual,
    queries_wide,
    keys_wide,
    values_wide,
    queries_narrow,
    keys_narrow,
    values_narrow,
    query_gain_wide,
    key_gain_wide,
    query_gain_narrow,
    key_gain_narrow,
    output_wide,
    output_narrow,
    norm_gain,
    gate_weight,
    up_weight,
    down_weight,
    route_ids,
    route_weights,
):
    n_sp, n_tp = lax.axis_size("sp"), lax.axis_size("tp")
    sp = lax.axis_index("sp")
    tok_count, own_rows = queries_wide.shape[0], residual.shape[0]
    model_width = residual.shape[1]
    hidden_width = gate_weight.shape[2]
    lanes = query_gain_wide.shape[0]
    tokens = n_sp * tok_count
    order = [r for r in range(n_tp) if r % 2 == 0] + [r for r in range(n_tp) if r % 2]
    half = tok_count // 2

    def across(value, axis, step):
        size = lax.axis_size(axis)
        return lax.ppermute(value, axis, [(i, i ^ step) for i in range(size)])

    def spread(own):
        two = across(own, "sp", 2)
        one = across(own, "sp", 1)
        return [own, one, two, across(two, "sp", 1)]

    def joined(first, second, axis):
        least = jnp.array(-jnp.inf, first.dtype)
        after, before = [(0, 0, 0)] * 2, [(0, 0, 0)] * 2
        after[axis], before[axis] = (0, second.shape[axis], 0), (first.shape[axis], 0, 0)
        return jnp.maximum(lax.pad(first, least, after), lax.pad(second, least, before))

    raw_wide = spread(joined(keys_wide, values_wide, 0))
    raw_narrow = spread(jnp.concatenate([keys_narrow.T, values_narrow.T], axis=0))

    table = like(tokens, lanes, jnp.float32)
    small = jnp.concatenate(
        [query_gain_wide, query_gain_narrow, query_gain_narrow]
        + [key_gain_wide, key_gain_narrow, key_gain_narrow]
        + [lane_freqs(lanes, lanes), lane_freqs(lanes // 2, lanes)]
    ).reshape(6, lanes)
    q_wide, q_narrow, *tables = on_core(
        functools.partial(prepare_kernel, order, own_rows),
        [like(*queries_wide.shape), like(*queries_narrow.shape)] + [table] * 4,
        [joined(queries_wide, queries_narrow, 1), small],
        flops=WAIT_FLOPS,
    )
    near, far = tuple(range(n_sp - 1)), (n_sp - 1,)
    parts = {
        "wide": (WIDE, raw_wide, [q_wide, small] + tables[:2], output_wide),
        "narrow": (NARROW, raw_narrow, [q_narrow, small] + tables[2:], output_narrow),
    }
    cost = dict(flops=WAIT_FLOPS // 2, exps=4 * tok_count**2)
    states = {}
    for name, (kind, raw, shared, _) in parts.items():
        heads = shared[0].shape[1] // lanes * kind[2]
        states[name] = on_core(
            functools.partial(attend_first_kernel, kind, near),
            [
                like(tok_count, lanes, jnp.float32),
                jax.ShapeDtypeStruct((heads, tok_count, lanes), jnp.float32),
            ],
            raw[:-1] + shared,
            **cost,
        )
    outs, terms = [like(tok_count, model_width, jnp.float32)], []
    for name, (kind, raw, shared, proj) in parts.items():
        terms = on_core(
            functools.partial(attend_last_kernel, kind, far),
            outs,
            [*raw[-1:], *shared, *states[name], proj, *terms],
            **cost,
        )
        outs = [like(half, model_width)] * 2
    keep, send = terms
    came = across(send, "tp", 1)

    experts = sp ^ jnp.arange(n_sp, dtype=route_ids.dtype)
    chosen = route_ids[:, :, None] == experts[None, None, :]
    own_weights = jnp.sum(jnp.where(chosen, route_weights[:, :, None], 0.0), axis=1)
    own_weights = lax.optimization_barrier((own_weights, send))[0]
    pair_weights = jnp.concatenate([own_weights, across(own_weights, "tp", 2)], axis=0)

    def crossing(keep, came):
        pair = keep[own_rows:].astype(jnp.float32) + came[own_rows:].astype(jnp.float32)
        return across(pair.astype(jnp.bfloat16), "tp", 2)

    attended, normed = on_core(
        norm_kernel,
        [like(own_rows, model_width)] * 2,
        [residual, keep, came, crossing(keep, came), norm_gain[None, :]],
        flops=WAIT_FLOPS,
    )

    arrived = spread(normed)
    crossed_rows, keeps, cames = [], [], []
    for r in range(n_sp):
        if r % 2:
            crossed_rows.append(across(crossed_rows[r - 1], "sp", 1))
        else:
            crossed_rows.append(across(arrived[r], "tp", 2))
        rows = [arrived[r], crossed_rows[r]]
        rows = rows + [across(rows[0], "tp", 1), across(rows[1], "tp", 1)]
        keep, send = on_core(
            expert_kernel,
            [like(half, model_width)] * 2,
            rows + [gate_weight, up_weight, down_weight],
            flops=6 * tok_count * model_width * hidden_width,
            exps=tok_count * hidden_width,
            vmem=12,
        )
        keeps.append(keep)
        cames.append(across(send, "tp", 1))

    def over_cores(r, rows=slice(None)):
        return keeps[r][rows].astype(jnp.float32) + cames[r][rows].astype(jnp.float32)

    beside = across(over_cores(1).astype(jnp.bfloat16), "sp", 1)
    gates, far_outs = [], []
    for r in range(2, n_sp):
        theirs = over_cores(r, slice(own_rows, None)).astype(jnp.bfloat16)
        crossed = across(theirs, "tp", 2).astype(jnp.float32)
        expert_out = (over_cores(r, slice(own_rows)) + crossed).astype(jnp.bfloat16)
        gates += [theirs] if far_outs else [theirs, expert_out]
        far_outs.append(across(expert_out, "sp", r).astype(jnp.float32))

    beside = lax.optimization_barrier((beside, *gates))[0].astype(jnp.float32)
    near_sum = over_cores(0) * pair_weights[:, 0:1] + beside * pair_weights[:, 1:2]
    crossed = across(near_sum[own_rows:].astype(jnp.bfloat16), "tp", 2)
    total = attended.astype(jnp.float32) + near_sum[:own_rows] + crossed.astype(jnp.float32)
    for r, expert_out in enumerate(far_outs, 2):
        total = total + pair_weights[:own_rows, r : r + 1] * expert_out
    return total.astype(jnp.bfloat16)


def body(*arrays):
    own_rows, pick_count = arrays[17].shape
    slot_count = 2 * pick_count * own_rows // lax.axis_size("sp")
    every_row_fits = slot_count >= own_rows and lax.axis_size("sp") == lax.axis_size("tp") == 4
    wide, narrow = arrays[7].shape[0], arrays[9].shape[0]
    one_key_head = arrays[2].shape[1] == wide and arrays[5].shape[1] == narrow
    full_lanes = wide == 128 and 2 * narrow == wide and arrays[4].shape[1] == wide
    whole_rows = arrays[1].shape[0] % GRID == 0 and own_rows % 8 == 0
    if every_row_fits and one_key_head and full_lanes and whole_rows:
        return dense_body(*arrays)
    return routed_body(*arrays)


def solution(mesh):
    return jax.shard_map(
        body,
        mesh=mesh,
        in_specs=(
            P(("grp", "sp", "tp"), None),
            P(("grp", "sp"), "tp"),
            P(("grp", "sp"), "tp"),
            P(("grp", "sp"), "tp"),
            P(("grp", "sp"), "tp"),
            P(("grp", "sp"), "tp"),
            P(("grp", "sp"), "tp"),
            P(),
            P(),
            P(),
            P(),
            P("tp", None),
            P("tp", None),
            P(),
            P("sp", None, "tp"),
            P("sp", None, "tp"),
            P("sp", "tp", None),
            P(("grp", "sp", "tp"), None),
            P(("grp", "sp", "tp"), None),
        ),
        out_specs=P(("grp", "sp", "tp"), None),
        check_vma=False,
    )
```

```python
import functools

import jax
import jax.numpy as jnp
import numpy as np
from jax import lax
from jax.experimental import pallas as pl
from jax.experimental.pallas import tpu as pltpu
from jax.sharding import PartitionSpec as P

GRID = 64


THETA = 10000.0
EPS = 1e-06
NEG_BIG = -1e30


def rotary_tables(places, head_width):
    quarter = head_width // 4
    inv_freq = THETA ** (-jnp.arange(quarter, dtype=jnp.float32) / quarter)
    grid_rows = (places // GRID).astype(jnp.float32)
    grid_cols = (places % GRID).astype(jnp.float32)
    row_angle = grid_rows[:, None] * inv_freq[None, :]
    col_angle = grid_cols[:, None] * inv_freq[None, :]
    angles = jnp.concatenate([row_angle, row_angle, col_angle, col_angle], axis=-1)
    return (jnp.cos(angles), jnp.sin(angles))


def head_norm_rotate(values, gain_vec, cos_table, sin_table):
    as_float = values.astype(jnp.float32)
    scaled = as_float * lax.rsqrt(jnp.mean(as_float * as_float, axis=-1, keepdims=True) + EPS)
    scaled = scaled * gain_vec
    full_shape = scaled.shape
    quarter = full_shape[-1] // 4
    halves = scaled.reshape(full_shape[:-1] + (2, 2, quarter))
    turned = jnp.stack([-halves[..., 1, :], halves[..., 0, :]], axis=-2).reshape(full_shape)
    return (scaled * cos_table[:, None, :] + turned * sin_table[:, None, :]).astype(jnp.bfloat16)


def fresh_state(queries):
    key_heads, group_size, tok_count = (queries.shape[1], queries.shape[2], queries.shape[0])
    return (
        jnp.full((key_heads, group_size, tok_count), NEG_BIG, jnp.float32),
        jnp.zeros((key_heads, group_size, tok_count), jnp.float32),
        jnp.zeros(queries.shape, jnp.float32),
    )


def key_sweep(carried, queries, keys, values):
    key_count = keys.shape[0]
    key_heads = queries.shape[1]
    head_width = queries.shape[3]
    block_len = 2048 if key_count % 2048 == 0 else key_count
    key_blocks = keys.reshape(key_count // block_len, block_len, key_heads, head_width)
    value_blocks = values.reshape(key_count // block_len, block_len, key_heads, head_width)
    score_scale = head_width ** (-0.5)

    def step(carried_state, blocks_in):
        key_block, value_block = blocks_in
        running_max, weight_sum, weighted = carried_state
        scores = (
            jnp.einsum("qhgd,khd->hgqk", queries, key_block, preferred_element_type=jnp.float32)
            * score_scale
        )
        new_max = jnp.maximum(running_max, jnp.max(scores, axis=-1))
        weights = jnp.exp(scores - new_max[..., None])
        rescale = jnp.exp(running_max - new_max)
        weight_sum = weight_sum * rescale + jnp.sum(weights, axis=-1)
        mixed_values = jnp.einsum(
            "hgqk,khd->qhgd",
            weights.astype(jnp.bfloat16),
            value_block,
            preferred_element_type=jnp.float32,
        )
        weighted = weighted * jnp.transpose(rescale, (2, 0, 1))[..., None] + mixed_values
        return ((new_max, weight_sum, weighted), None)

    carried, _ = lax.scan(step, carried, (key_blocks, value_blocks))
    return carried


def finish_heads(carried):
    weighted = carried[2]
    outcome = weighted / jnp.transpose(carried[1], (2, 0, 1))[..., None]
    return outcome.astype(jnp.bfloat16).reshape(weighted.shape[0], -1)


def slot_tables(chosen, slot_count, expert_count):
    row_count = chosen.shape[0]
    pick_count = chosen.shape[1]
    flat_pick = chosen.reshape(row_count * pick_count)
    hit_marks = (flat_pick[:, None] == jnp.arange(expert_count, dtype=jnp.int32)[None, :]).astype(
        jnp.int32
    )
    before = jnp.cumsum(hit_marks, axis=0) - hit_marks
    slot_place = jnp.sum(before * hit_marks, axis=1)
    target = flat_pick * slot_count + slot_place
    slot_table = target[:, None] == jnp.arange(expert_count * slot_count, dtype=jnp.int32)[None, :]
    return slot_table.astype(jnp.bfloat16).reshape(row_count, pick_count, expert_count * slot_count)


def routed_body(
    residual,
    queries_wide,
    keys_wide,
    values_wide,
    queries_narrow,
    keys_narrow,
    values_narrow,
    query_gain_wide,
    key_gain_wide,
    query_gain_narrow,
    key_gain_narrow,
    output_wide,
    output_narrow,
    norm_gain,
    gate_weight,
    up_weight,
    down_weight,
    route_ids,
    route_weights,
):
    tok_count = queries_wide.shape[0]
    places = lax.axis_index("sp") * tok_count + jnp.arange(tok_count, dtype=jnp.int32)
    wide_width = query_gain_wide.shape[0]
    narrow_width = query_gain_narrow.shape[0]
    cos_wide, sin_wide = rotary_tables(places, wide_width)
    cos_narrow, sin_narrow = rotary_tables(places, narrow_width)
    wide_keyheads = keys_wide.shape[1] // wide_width
    narrow_keyheads = keys_narrow.shape[1] // narrow_width
    q_wide = head_norm_rotate(
        queries_wide.reshape(tok_count, -1, wide_width), query_gain_wide, cos_wide, sin_wide
    )
    q_wide = q_wide.reshape(tok_count, wide_keyheads, -1, wide_width)
    k_wide = head_norm_rotate(
        keys_wide.reshape(tok_count, -1, wide_width), key_gain_wide, cos_wide, sin_wide
    )
    k_wide = k_wide.reshape(tok_count, -1)
    q_narrow = head_norm_rotate(
        queries_narrow.reshape(tok_count, -1, narrow_width),
        query_gain_narrow,
        cos_narrow,
        sin_narrow,
    )
    q_narrow = q_narrow.reshape(tok_count, narrow_keyheads, -1, narrow_width)
    k_narrow = head_norm_rotate(
        keys_narrow.reshape(tok_count, -1, narrow_width), key_gain_narrow, cos_narrow, sin_narrow
    )
    k_narrow = k_narrow.reshape(tok_count, -1)
    carried = (fresh_state(q_wide), fresh_state(q_narrow))
    carried = (
        key_sweep(
            carried[0],
            q_wide,
            lax.all_gather(k_wide, "sp", axis=0, tiled=True),
            lax.all_gather(values_wide, "sp", axis=0, tiled=True),
        ),
        key_sweep(
            carried[1],
            q_narrow,
            lax.all_gather(k_narrow, "sp", axis=0, tiled=True),
            lax.all_gather(values_narrow, "sp", axis=0, tiled=True),
        ),
    )
    heads_wide = finish_heads(carried[0])
    heads_narrow = finish_heads(carried[1])
    own_rows = residual.shape[0]
    mixed_heads = lax.psum_scatter(
        (
            jnp.dot(heads_wide, output_wide, preferred_element_type=jnp.float32)
            + jnp.dot(heads_narrow, output_narrow, preferred_element_type=jnp.float32)
        ).astype(jnp.bfloat16),
        "tp",
        scatter_dimension=0,
        tiled=True,
    ).astype(jnp.float32)
    attended = (residual.astype(jnp.float32) + mixed_heads).astype(jnp.bfloat16)
    state_float = attended.astype(jnp.float32)
    normed = (
        state_float
        * lax.rsqrt(jnp.mean(state_float * state_float, axis=-1, keepdims=True) + EPS)
        * norm_gain
    ).astype(jnp.bfloat16)
    pick_count = route_ids.shape[1]
    expert_count = lax.axis_size("sp")
    slot_count = 2 * pick_count * own_rows // expert_count
    model_width = residual.shape[1]
    own_tables = slot_tables(route_ids, slot_count, expert_count)
    send_rows = jnp.einsum(
        "rks,rd->sd", own_tables, normed, preferred_element_type=jnp.float32
    ).astype(jnp.bfloat16)
    send_rows = send_rows.reshape(expert_count, slot_count, model_width)
    arrived = lax.all_to_all(send_rows, "sp", split_axis=0, concat_axis=0, tiled=True)
    copies = lax.all_gather(arrived, "tp", axis=0, tiled=True)
    expert_arrived = copies.reshape((lax.axis_size("tp"),) + arrived.shape)
    full_shape = expert_arrived.shape
    flat_rows = expert_arrived.reshape(-1, model_width)
    gate_act = jnp.dot(flat_rows, gate_weight[0], preferred_element_type=jnp.float32)
    up_act = jnp.dot(flat_rows, up_weight[0], preferred_element_type=jnp.float32)
    hidden = (jax.nn.silu(gate_act) * up_act).astype(jnp.bfloat16)
    partial_value = jnp.dot(hidden, down_weight[0], preferred_element_type=jnp.float32).reshape(
        full_shape
    )
    summed = lax.psum_scatter(
        partial_value.astype(jnp.bfloat16), "tp", scatter_dimension=0, tiled=True
    ).astype(jnp.float32)
    results = summed.reshape(full_shape[1:]).astype(jnp.bfloat16)
    returned = lax.all_to_all(results, "sp", split_axis=0, concat_axis=0, tiled=True)
    returned_flat = returned.reshape(expert_count * slot_count, model_width)
    picked = jnp.einsum(
        "rks,sd->rkd", own_tables, returned_flat, preferred_element_type=jnp.float32
    )
    mixture = jnp.sum(route_weights[:, :, None] * picked, axis=1)
    return (state_float + mixture).astype(jnp.bfloat16)


VMEM_SPEC = pl.BlockSpec(memory_space=pltpu.VMEM)
MIB = 2**20
WAIT_FLOPS = 8 * 10**9


def on_core(kernel, results, args, flops=0, exps=0, vmem=16):
    moved = sum(a.size * a.dtype.itemsize for a in list(args) + list(results))
    return pl.pallas_call(
        kernel,
        out_shape=results,
        in_specs=[VMEM_SPEC] * len(args),
        out_specs=[VMEM_SPEC] * len(results),
        compiler_params=pltpu.CompilerParams(vmem_limit_bytes=vmem * MIB),
        cost_estimate=pl.CostEstimate(
            flops=int(flops), bytes_accessed=int(moved), transcendentals=int(exps)
        ),
    )(*args)


def like(rows, cols, dtype=jnp.bfloat16):
    return jax.ShapeDtypeStruct((rows, cols), dtype)


def lanes_of(shape):
    return lax.broadcasted_iota(jnp.int32, shape, 1)


def turned(values, quarter):
    width = values.shape[1]
    ahead = pltpu.roll(values, width - quarter, 1)
    behind = pltpu.roll(values, quarter, 1)
    return jnp.where(lanes_of(values.shape) % (2 * quarter) < quarter, ahead, behind)


def rotated(scaled, quarter, cos_table, sin_table):
    return (scaled * cos_table + turned(scaled, quarter) * sin_table).astype(jnp.bfloat16)


def rms(values, width):
    return lax.rsqrt(jnp.sum(values * values, axis=1, keepdims=True) / width + EPS)


def prepare_kernel(
    order,
    own_rows,
    query_ref,
    small_ref,
    qw_out,
    qn_out,
    cw_ref,
    sw_ref,
    cn_ref,
    sn_ref,
):
    tokens, lanes = cw_ref.shape
    grid_rows = tokens // GRID
    for freq, width, cos_ref, sin_ref in (
        (small_ref[4:5, :], lanes, cw_ref, sw_ref),
        (small_ref[5:6, :], lanes // 2, cn_ref, sn_ref),
    ):
        row_at = lax.broadcasted_iota(jnp.int32, (grid_rows, lanes), 0).astype(jnp.float32) * freq
        col_at = lax.broadcasted_iota(jnp.int32, (GRID, lanes), 0).astype(jnp.float32) * freq
        quarter = width // 4
        row_cos, row_sin = jnp.cos(row_at), jnp.sin(row_at)
        col_cos, col_sin = jnp.cos(col_at), jnp.sin(col_at)
        lane = lanes_of((GRID, lanes))
        minus = lane % (2 * quarter) < quarter
        by_row = lane % width < width // 2
        for i in range(grid_rows):
            here = pl.ds(i * GRID, GRID)
            cos_ref[here, :] = jnp.where(by_row, row_cos[i : i + 1, :], col_cos)
            sines = jnp.where(by_row, row_sin[i : i + 1, :], col_sin)
            sin_ref[here, :] = jnp.where(minus, -sines, sines)
    sp, tp = lax.axis_index("sp"), lax.axis_index("tp")
    count = len(order) * own_rows
    gain_wide, gain_narrow = small_ref[0:1, :], small_ref[1:2, :]
    for slot, r in enumerate(order):
        source = pl.ds(pl.multiple_of((tp ^ r) * own_rows, own_rows), own_rows)
        place = pl.ds(pl.multiple_of(sp * count + (tp ^ r) * own_rows, own_rows), own_rows)
        target = pl.ds(slot * own_rows, own_rows)
        for h in range(qw_out.shape[1] // lanes):
            head = pl.ds(h * lanes, lanes)
            value = query_ref[source, head].astype(jnp.float32)
            value = value * rms(value, lanes) * gain_wide
            qw_out[target, head] = rotated(value, lanes // 4, cw_ref[place, :], sw_ref[place, :])
        value = query_ref[source, qw_out.shape[1] :].astype(jnp.float32)
        low = lanes_of(value.shape) < lanes // 2
        first = rms(jnp.where(low, value, 0.0), lanes // 2)
        second = rms(jnp.where(low, 0.0, value), lanes // 2)
        value = value * jnp.where(low, first, second) * gain_narrow
        qn_out[target, :] = rotated(value, lanes // 8, cn_ref[place, :], sn_ref[place, :])


def mixed_in(query, keys, values, scale, before=None):
    scores = lax.dot_general(
        query, keys, (((1,), (1,)), ((), ())), preferred_element_type=jnp.float32
    )
    top = jnp.max(scores, axis=1, keepdims=True)
    if before is not None:
        top = jnp.maximum(top, before[0])
    weights = jnp.exp((scores - top) * scale)
    total = jnp.sum(weights, axis=1, keepdims=True)
    mixed = jnp.dot(weights.astype(jnp.bfloat16), values, preferred_element_type=jnp.float32)
    if before is not None:
        fade = jnp.exp((before[0] - top) * scale)
        total = total + before[1] * fade
        mixed = mixed + before[2] * fade
    return top, total, mixed


def wide_keys(raw_refs, steps, small_ref, cos_ref, sin_ref):
    lanes = small_ref.shape[1]
    sp = lax.axis_index("sp")
    keys, values = [], []
    for r, ref in zip(steps, raw_refs, strict=True):
        count = ref.shape[0] // 2
        place = pl.ds(pl.multiple_of((sp ^ r) * count, count), count)
        value = ref[:count, :].astype(jnp.float32)
        value = value * rms(value, lanes) * small_ref[2:3, :]
        keys.append(rotated(value, lanes // 4, cos_ref[place, :], sin_ref[place, :]))
        values.append(ref[count:, :])
    return jnp.concatenate(keys, axis=0), jnp.concatenate(values, axis=0)


def narrow_keys(raw_refs, steps, small_ref, cos_ref, sin_ref):
    lanes = small_ref.shape[1]
    sp = lax.axis_index("sp")
    keys, values = [], []
    for r, ref in zip(steps, raw_refs, strict=True):
        count = ref.shape[1]
        place = pl.ds(pl.multiple_of((sp ^ r) * count, count), count)
        both = ref[...].astype(jnp.float32).T
        low = lanes_of(both.shape) < lanes // 2
        other = pltpu.roll(both, lanes // 2, 1)
        value = jnp.where(low, both, other)
        value = value * rms(jnp.where(low, both, 0.0), lanes // 2) * small_ref[3:4, :]
        keys.append(rotated(value, lanes // 8, cos_ref[place, :], sin_ref[place, :]))
        values.append(jnp.where(low, other, both).astype(jnp.bfloat16))
    return jnp.concatenate(keys, axis=0), jnp.concatenate(values, axis=0)


def wide_queries(ref, lanes):
    return [ref[:, h * lanes : (h + 1) * lanes] for h in range(ref.shape[1] // lanes)]


def narrow_queries(ref, lanes):
    query = ref[...]
    low = lanes_of(query.shape) < lanes // 2
    nothing = jnp.zeros_like(query)
    return [jnp.where(low, query, nothing), jnp.where(low, nothing, query)]


WIDE = (wide_keys, wide_queries, 1)
NARROW = (narrow_keys, narrow_queries, 2)


def attend_first_kernel(kind, steps, *refs):
    raw_refs, refs = refs[: len(steps)], refs[len(steps) :]
    query_ref, small_ref, cos_ref, sin_ref, stat_ref, mixed_ref = refs
    lanes = small_ref.shape[1]
    keys, values = kind[0](raw_refs, steps, small_ref, cos_ref, sin_ref)
    scale = (lanes // kind[2]) ** -0.5
    lane = lanes_of(stat_ref.shape)
    stat = jnp.zeros(stat_ref.shape, jnp.float32)
    for h, query in enumerate(kind[1](query_ref, lanes)):
        top, total, mixed = mixed_in(query, keys, values, scale)
        stat = jnp.where(lane == 2 * h, top, stat)
        stat = jnp.where(lane == 2 * h + 1, total, stat)
        mixed_ref[h] = mixed
    stat_ref[...] = stat


def attend_last_kernel(kind, steps, row_sets, *refs):
    count = len(steps) or 2
    raw_refs, refs = refs[:count], refs[count:]
    query_ref, small_ref, cos_ref, sin_ref, stat_ref, mixed_ref, *refs = refs
    lanes = small_ref.shape[1]
    if steps:
        keys, values = kind[0](raw_refs, steps, small_ref, cos_ref, sin_ref)
    else:
        keys, values = [ref[...] for ref in raw_refs]
    scale = (lanes // kind[2]) ** -0.5
    queries = kind[1](query_ref, lanes)
    outs = refs if kind[2] == 1 else refs[3:]
    for rows, out_ref in zip(row_sets, outs):
        heads = []
        for h, query in enumerate(queries):
            top, total = stat_ref[rows, 2 * h : 2 * h + 1], stat_ref[rows, 2 * h + 1 : 2 * h + 2]
            before = (top, total, mixed_ref[h, rows])
            _, total, mixed = mixed_in(query[rows], keys, values, scale, before)
            heads.append(mixed / total)
        if kind[2] == 1:
            out_ref[...] = jnp.concatenate(heads, axis=1).astype(jnp.bfloat16)
            continue
        wide_ref, wide_proj_ref, narrow_proj_ref = refs[:3]
        narrow = jnp.where(lanes_of(heads[0].shape) < lanes // 2, heads[0], heads[1])
        terms = jnp.dot(wide_ref[rows, :], wide_proj_ref[...], preferred_element_type=jnp.float32)
        terms = terms + jnp.dot(
            narrow.astype(jnp.bfloat16), narrow_proj_ref[...], preferred_element_type=jnp.float32
        )
        out_ref[...] = terms.astype(jnp.bfloat16)
    for value, ref in zip((keys, values), outs[len(row_sets) :]):
        ref[...] = value


def norm_kernel(res_ref, keep_ref, came_ref, crossed_ref, gain_ref, att_ref, normed_ref):
    rows = res_ref.shape[0]
    term = keep_ref[:rows, :].astype(jnp.float32) + came_ref[:rows, :].astype(jnp.float32)
    term = term + crossed_ref[...].astype(jnp.float32)
    attended = (res_ref[...].astype(jnp.float32) + term).astype(jnp.bfloat16)
    att_ref[...] = attended
    state = attended.astype(jnp.float32)
    normed_ref[...] = (state * rms(state, state.shape[1]) * gain_ref[...]).astype(jnp.bfloat16)


def expert_kernel(ours_ref, theirs_ref, gate_ref, up_ref, down_ref, keep_ref, send_ref):
    rows = jnp.concatenate([ours_ref[...], theirs_ref[...]], axis=0)
    gate_act = jnp.dot(rows, gate_ref[0], preferred_element_type=jnp.float32)
    up_act = jnp.dot(rows, up_ref[0], preferred_element_type=jnp.float32)
    hidden = (gate_act / (1.0 + jnp.exp(-gate_act)) * up_act).astype(jnp.bfloat16)
    piece = jnp.dot(hidden, down_ref[0], preferred_element_type=jnp.float32).astype(jnp.bfloat16)
    half = ours_ref.shape[0]
    keep_ref[...] = piece[:half]
    send_ref[...] = piece[half:]


def lane_freqs(width, lanes):
    quarter = width // 4
    freq = THETA ** (-np.arange(quarter, dtype=np.float64) / quarter)
    return jnp.asarray(np.tile(freq, lanes // quarter), jnp.float32)


def dense_body(
    residual,
    queries_wide,
    keys_wide,
    values_wide,
    queries_narrow,
    keys_narrow,
    values_narrow,
    query_gain_wide,
    key_gain_wide,
    query_gain_narrow,
    key_gain_narrow,
    output_wide,
    output_narrow,
    norm_gain,
    gate_weight,
    up_weight,
    down_weight,
    route_ids,
    route_weights,
):
    n_sp, n_tp = lax.axis_size("sp"), lax.axis_size("tp")
    sp = lax.axis_index("sp")
    tok_count, own_rows = queries_wide.shape[0], residual.shape[0]
    model_width = residual.shape[1]
    hidden_width = gate_weight.shape[2]
    lanes = query_gain_wide.shape[0]
    tokens = n_sp * tok_count
    order = [r for r in range(n_tp) if r % 2 == 0] + [r for r in range(n_tp) if r % 2]

    def across(value, axis, step):
        size = lax.axis_size(axis)
        return lax.ppermute(value, axis, [(i, i ^ step) for i in range(size)])

    def spread(own):
        two = across(own, "sp", 2)
        one = across(own, "sp", 1)
        return [own, one, two, across(two, "sp", 1)]

    def joined(first, second, axis):
        least = jnp.array(-jnp.inf, first.dtype)
        after, before = [(0, 0, 0)] * 2, [(0, 0, 0)] * 2
        after[axis], before[axis] = (0, second.shape[axis], 0), (first.shape[axis], 0, 0)
        return jnp.maximum(lax.pad(first, least, after), lax.pad(second, least, before))

    raw_wide = spread(joined(keys_wide, values_wide, 0))
    raw_narrow = spread(jnp.concatenate([keys_narrow.T, values_narrow.T], axis=0))

    table = like(tokens, lanes, jnp.float32)
    small = jnp.concatenate(
        [query_gain_wide, query_gain_narrow, query_gain_narrow]
        + [key_gain_wide, key_gain_narrow, key_gain_narrow]
        + [lane_freqs(lanes, lanes), lane_freqs(lanes // 2, lanes)]
    ).reshape(6, lanes)
    q_wide, q_narrow, *tables = on_core(
        functools.partial(prepare_kernel, order, own_rows),
        [like(*queries_wide.shape), like(*queries_narrow.shape)] + [table] * 4,
        [joined(queries_wide, queries_narrow, 1), small],
        flops=WAIT_FLOPS,
    )
    near, far = tuple(range(n_sp - 1)), (n_sp - 1,)
    parts = {
        "wide": (WIDE, raw_wide, [q_wide, small] + tables[:2]),
        "narrow": (NARROW, raw_narrow, [q_narrow, small] + tables[2:]),
    }
    cost = dict(flops=WAIT_FLOPS // 2, exps=4 * tok_count**2)
    states = {}
    for name, (kind, raw, shared) in parts.items():
        heads = shared[0].shape[1] // lanes * kind[2]
        states[name] = on_core(
            functools.partial(attend_first_kernel, kind, near),
            [
                like(tok_count, lanes, jnp.float32),
                jax.ShapeDtypeStruct((heads, tok_count, lanes), jnp.float32),
            ],
            raw[:-1] + shared,
            **cost,
        )

    def last(name, row_sets, outs, extra, ready=None):
        kind, raw, shared = parts[name]
        steps, given = ((), ready) if ready else (far, raw[-1:])
        return on_core(
            functools.partial(attend_last_kernel, kind, steps, row_sets),
            outs,
            [*given, *shared, *states[name], *extra],
            **cost,
        )

    ours, far_ours, others, far_others = [
        slice(i * own_rows, (i + 1) * own_rows) for i in range(n_tp)
    ]
    wide = last("wide", [slice(None)], [like(*queries_wide.shape)], [])
    extra, out = [*wide, output_wide, output_narrow], like(own_rows, model_width)
    made = [like(tok_count, lanes)] * 2
    send_far, *ready = last("narrow", [far_others], [out] + made, extra)
    came_far = across(send_far, "tp", 1)
    keep_far = last("narrow", [far_ours], [out], extra, ready)[0]
    pair = keep_far.astype(jnp.float32) + came_far.astype(jnp.float32)
    crossed = across(pair.astype(jnp.bfloat16), "tp", 2)
    send, keep = last("narrow", [others, ours], [out] * 2, extra, ready)
    came = across(send, "tp", 1)

    experts = sp ^ jnp.arange(n_sp, dtype=route_ids.dtype)
    chosen = route_ids[:, :, None] == experts[None, None, :]
    own_weights = jnp.sum(jnp.where(chosen, route_weights[:, :, None], 0.0), axis=1)
    own_weights = lax.optimization_barrier((own_weights, keep))[0]
    beside_weights = across(own_weights, "tp", 2)

    attended, normed = on_core(
        norm_kernel,
        [like(own_rows, model_width)] * 2,
        [residual, keep, came, crossed, norm_gain[None, :]],
        flops=WAIT_FLOPS,
    )

    arrived = spread(normed)

    def expert_parts(rows):
        other = across(rows, "tp", 1)
        keep, send = on_core(
            expert_kernel,
            [like(own_rows, model_width)] * 2,
            [rows, other, gate_weight, up_weight, down_weight],
            flops=3 * tok_count * model_width * hidden_width,
            exps=tok_count * hidden_width // 2,
            vmem=12,
        )
        came = across(send, "tp", 1)
        return keep.astype(jnp.float32) + came.astype(jnp.float32)

    crossed_rows, ours, theirs = [], [], []
    for r in range(n_sp):
        if r % 2:
            crossed_rows.append(across(crossed_rows[r - 1], "sp", 1))
        else:
            crossed_rows.append(across(arrived[r], "tp", 2))
        ours.append(expert_parts(arrived[r]))
        theirs.append(expert_parts(crossed_rows[r]))

    near = [across(v[1].astype(jnp.bfloat16), "sp", 1) for v in (ours, theirs)]
    gates, far_outs = [], []
    for r in range(2, n_sp):
        sent = theirs[r].astype(jnp.bfloat16)
        crossed = across(sent, "tp", 2).astype(jnp.float32)
        outcome = (ours[r] + crossed).astype(jnp.bfloat16)
        gates += [sent] if r > 2 else [sent, outcome]
        far_outs.append(across(outcome, "sp", r).astype(jnp.float32))

    near = [v.astype(jnp.float32) for v in lax.optimization_barrier((*near, *gates))[:2]]
    sent = theirs[0] * beside_weights[:, 0:1] + near[1] * beside_weights[:, 1:2]
    crossed = across(sent.astype(jnp.bfloat16), "tp", 2).astype(jnp.float32)
    total = attended.astype(jnp.float32) + crossed
    total = total + ours[0] * own_weights[:, 0:1] + near[0] * own_weights[:, 1:2]
    for r, expert_out in enumerate(far_outs, 2):
        total = total + own_weights[:, r : r + 1] * expert_out
    return total.astype(jnp.bfloat16)


def body(*arrays):
    own_rows, pick_count = arrays[17].shape
    slot_count = 2 * pick_count * own_rows // lax.axis_size("sp")
    every_row_fits = slot_count >= own_rows and lax.axis_size("sp") == lax.axis_size("tp") == 4
    wide, narrow = arrays[7].shape[0], arrays[9].shape[0]
    one_key_head = arrays[2].shape[1] == wide and arrays[5].shape[1] == narrow
    full_lanes = wide == 128 and 2 * narrow == wide and arrays[4].shape[1] == wide
    whole_rows = arrays[1].shape[0] % GRID == 0 and own_rows % 8 == 0
    if every_row_fits and one_key_head and full_lanes and whole_rows:
        return dense_body(*arrays)
    return routed_body(*arrays)


def solution(mesh):
    return jax.shard_map(
        body,
        mesh=mesh,
        in_specs=(
            P(("grp", "sp", "tp"), None),
            P(("grp", "sp"), "tp"),
            P(("grp", "sp"), "tp"),
            P(("grp", "sp"), "tp"),
            P(("grp", "sp"), "tp"),
            P(("grp", "sp"), "tp"),
            P(("grp", "sp"), "tp"),
            P(),
            P(),
            P(),
            P(),
            P("tp", None),
            P("tp", None),
            P(),
            P("sp", None, "tp"),
            P("sp", None, "tp"),
            P("sp", "tp", None),
            P(("grp", "sp", "tp"), None),
            P(("grp", "sp", "tp"), None),
        ),
        out_specs=P(("grp", "sp", "tp"), None),
        check_vma=False,
    )
```
